32 devices in a mesh: grp: 2 (over y), ep: 16 (over z, x, core), tp: 1.
Axes of the slice: x: 2, y: 2, z: 4, core: 2. Of those that a mesh axis runs over, the one named last changes fastest.
Arguments:
- tokens: bfloat16 [2048, 2048], P(('grp', 'ep')), parts along dimension 0, may hold values from -6 to 6
- norm_gain: float32 [2048], replicated, may hold values from 0.1 to 1.9
- routes: int32 [2048, 6], P(('grp', 'ep')), parts along dimension 0, may hold values from 0 to 15, all different within a row; in each aligned block of 64 rows (0 to 63, 64 to 127, ...) at most 48 rows name the same one
- route_weights: float32 [2048, 6], P(('grp', 'ep')), parts along dimension 0, may hold values from 0.05 to 1
- w_gate: bfloat16 [16, 2048, 2048], P('ep', None, 'tp'), may hold values from -0.125 to 0.125
- w_up: bfloat16 [16, 2048, 2048], P('ep', None, 'tp'), may hold values from -0.125 to 0.125
- w_down: bfloat16 [16, 2048, 2048], P('ep', 'tp'), may hold values from -4 to 4
- final_gain: float32 [2048], P('tp'), may hold values from 0.1 to 1.9
Outputs:
- mixed_out: bfloat16 [2048, 2048], P(('grp', 'ep'), 'tp'), parts along dimension 0
The draws below stay inside these ranges and needn't reach their ends.
There are 2 independent parts, one for each index of `grp`. The reference program is written for one: setup_inputs(seed, part) draws one part's arguments, and reference() takes and returns one part's arrays. A program takes and returns all parts, laid end to end along the dimension named above; an argument that names none is the same for every part. Nothing has to cross between parts.
Inputs may be any that keep to these rules, and one draw needn't show every extreme that they name: `routes`: each row names 6 different experts; within the rows of one index of ep no expert is named by more than 48 rows, and in every draw some expert is named by exactly 48 rows of some index.
All inputs are finite; a program needn't handle non-finite values.
Results may differ from the reference program's by a relative error of at most 0.015.
Values may be sent and summed in bfloat16 or wider, within the bound.
A program may use at most 64 MiB of HBM per device.

```python
import math
import jax
import jax.numpy as jnp
import numpy as np
from jax import lax

D = 2048
FF = 2048
TOP_K = 6
TOK_DEV = 64
EXPERTS = 16
CAP = 48
TOKENS = 1024
N_EP = 16
N_TP = 1


def draw_w_down(key, part):
    key_values, key_columns = jax.random.split(key)
    columns = jnp.arange(D, dtype=jnp.float32) / D
    roughness = jax.random.uniform(key_columns, (D,), jnp.float32, 0.5, 1.5)
    values = jnp.clip(jax.random.normal(key_values, (EXPERTS, FF, D), jnp.float32), -5.0, 5.0)
    column_scale = jnp.exp(columns * jnp.log(10.0)) * roughness
    scaled = values * column_scale[None, None, :] * FF ** (-0.5) / 3.0
    return scaled.astype(jnp.bfloat16)


def block_scale(own_key, shape, cuts, smallest, high):
    loudness, own = 1.0, jax.random.fold_in(own_key, 6)
    for position, blocks in cuts:
        steps = jnp.exp(jax.random.uniform(jax.random.fold_in(own, position), (blocks,), jnp.float32, smallest / len(cuts), high / len(cuts)))
        loudness = loudness * jnp.repeat(steps, shape[position] // blocks).reshape([-1 if axis == position else 1 for axis in range(len(shape))])
    return loudness


def deal_out(key, own, number, rows, count, top, reach, slope):
    order = jax.random.permutation(key, count)
    crowded, common = load_shares(count, rows * top, reach, slope, True), load_shares(count, rows * top, reach, slope, False)
    places = jnp.arange(count)

    def named(sizes, offset_by):
        used = int((sizes > 0).sum())
        fixed = max(1, used // 4)
        shifted = fixed + (places - fixed + offset_by * (used - fixed)) % max(1, count - fixed)
        return jnp.zeros((count,), jnp.int32).at[order[jnp.where(places < fixed, places, shifted)]].set(jnp.asarray(sizes, jnp.int32))

    sizes = jnp.where(number % 4 == 0, named(crowded, number // 4), named(common, number - number // 4 - 1))
    mixed = jax.random.permutation(jax.random.fold_in(own, 3), count)
    source_of, taker = mixed[0:count // 2 * 2:2], mixed[1:count // 2 * 2:2]
    margin = jnp.minimum(sizes[source_of] - 1, reach - sizes[taker]) // 2
    margin = jnp.where((source_of == order[0]) | (taker == order[0]) | (sizes[taker] == 0), 0, jnp.maximum(margin, 0))
    shifted = jax.random.randint(jax.random.fold_in(own, 4), (count // 2,), 0, 1 << 20) % (margin + 1)
    sizes = sizes.at[source_of].add(-shifted).at[taker].add(shifted)
    labels = jnp.searchsorted(jnp.cumsum(sizes), jnp.arange(rows * top), side="right").astype(jnp.int32)
    listing = labels.reshape(top, rows).T
    listing = listing[jax.random.permutation(jax.random.fold_in(own, 1), rows)]
    offset_by = jax.random.randint(jax.random.fold_in(own, 2), (rows, 1), 0, top)
    return jnp.take_along_axis(listing, (jnp.arange(top)[None, :] + offset_by) % top, axis=1)


def load_shares(number_of, total, reach, slope, full):
    weights = [(1 << 20) // math.isqrt(standing ** slope) + 1 for standing in range(1, number_of + 1)]
    largest = reach if full else min(reach, max(-(-total // number_of), total * weights[0] // sum(weights)))
    least = 1 if total - largest >= number_of - 1 else 0
    counts, surplus = [largest] + [least] * (number_of - 1), total - largest - least * (number_of - 1)
    while surplus > 0:
        candidates = [i for i in range(1, number_of) if counts[i] < largest] or [i for i in range(1, number_of) if counts[i] < reach]
        mass, left = sum([weights[i] for i in candidates]), surplus
        for i in candidates:
            more = min(reach - counts[i], max(1, left * weights[i] // mass), surplus)
            counts[i] = counts[i] + more
            surplus = surplus - more
    return np.array(counts)


def scatter_about(rng, shape, deviation, bound, cuts=(), kind=jnp.bfloat16):
    loudness = block_scale(rng, shape, cuts, -0.22, 0.18) if cuts else 1.0
    array = jax.random.normal(rng, shape, jnp.float32) * deviation * loudness
    return jnp.minimum(jnp.maximum(array, -bound), bound).astype(kind)


def setup_inputs(seed: int = 0, part: int = 0) -> dict:
    keys = jax.random.split(jax.random.key(seed), 9)
    part_splits = jax.random.split(jax.random.fold_in(keys[8], part), 9)
    tokens = scatter_about(part_splits[0], (TOKENS, D), 1.0, 6.0, ((0, 16),))
    norm_gain = jnp.clip(1.0 + 0.18 * jax.random.normal(keys[1], (D,), jnp.float32), 0.1, 1.9)
    routes_keys = jax.random.split(jax.random.fold_in(part_splits[2], 1), TOKENS // TOK_DEV)
    routes_turns = jax.random.permutation(jax.random.fold_in(part_splits[2], 3), TOKENS // TOK_DEV)
    routes = jax.vmap(lambda own, number: deal_out(jax.random.fold_in(part_splits[2], 2), own, number, TOK_DEV, EXPERTS, TOP_K, CAP, 2))(routes_keys, routes_turns).reshape((TOKENS, TOP_K))
    route_weights = jnp.clip(jnp.exp(math.log(1.0) - 2.9957323 * jax.random.uniform(part_splits[3], (TOKENS, TOP_K), jnp.float32) ** block_scale(part_splits[3], (TOKENS, TOP_K), ((0, 16),), -0.2, 0.2)), 0.05, 1.0)
    w_gate = scatter_about(keys[4], (EXPERTS, D, FF), D ** -0.5, 0.125, ((0, 16),))
    w_up = scatter_about(keys[5], (EXPERTS, D, FF), D ** -0.5, 0.125, ((0, 16),))
    w_down = draw_w_down(jax.random.fold_in(keys[8], 71), part)
    final_gain = jnp.clip(1.0 + 0.18 * jax.random.normal(keys[7], (D,), jnp.float32), 0.1, 1.9)
    return dict(tokens=tokens, norm_gain=norm_gain, routes=routes, route_weights=route_weights, w_gate=w_gate, w_up=w_up, w_down=w_down, final_gain=final_gain)


EPS = 1e-06

def slot_table(route_rows):
    flattened = route_rows.reshape(-1)
    matches = (flattened[:, None] == jnp.arange(EXPERTS, dtype=jnp.int32)[None, :]).astype(jnp.int32)
    earlier = jnp.cumsum(matches, axis=0) - matches
    slot_of = lax.optimization_barrier(jnp.sum(earlier * matches, axis=1))
    return (flattened * CAP + slot_of).reshape(route_rows.shape).astype(jnp.int32)

def dispatch(place_block, row_block):
    slot_ids = jnp.arange(EXPERTS * CAP, dtype=jnp.int32)
    selector = lax.optimization_barrier(jnp.sum((place_block[None, :, :] == slot_ids[:, None, None]).astype(jnp.float32), axis=2))
    return jnp.dot(selector.astype(jnp.bfloat16), row_block, preferred_element_type=jnp.float32).astype(jnp.bfloat16)

def expert(inputs):
    row_block, gate_w, up_w, down_w = inputs
    gate_value = jnp.dot(row_block, gate_w, preferred_element_type=jnp.float32)
    up_value = jnp.dot(row_block, up_w, preferred_element_type=jnp.float32)
    hidden = (jax.nn.silu(gate_value) * up_value).astype(jnp.bfloat16)
    hidden_split = hidden.reshape(row_block.shape[0], N_TP, FF // N_TP).astype(jnp.float32)
    down_split = down_w.reshape(N_TP, FF // N_TP, D).astype(jnp.float32)
    partial_value = jnp.einsum('rjf,jfd->jrd', hidden_split, down_split).astype(jnp.bfloat16)
    partial_value = lax.optimization_barrier(partial_value)
    return lax.optimization_barrier(jnp.sum(partial_value.astype(jnp.float32), axis=0)).astype(jnp.bfloat16)

def reference(tokens, norm_gain, routes, route_weights, w_gate, w_up, w_down, final_gain):
    tokens_f = tokens.astype(jnp.float32)
    inverse = lax.rsqrt(lax.optimization_barrier(jnp.mean(tokens_f * tokens_f, axis=1, keepdims=True)) + EPS)
    normed = (tokens_f * inverse * norm_gain[None, :]).astype(jnp.bfloat16)
    blocks = normed.reshape(N_EP, TOK_DEV, D)
    places = jax.vmap(slot_table)(routes.reshape(N_EP, TOK_DEV, TOP_K))
    buffers = jax.vmap(dispatch)(places, blocks)
    expert_in = buffers.reshape(N_EP, EXPERTS, CAP, D).transpose(1, 0, 2, 3).reshape(EXPERTS, N_EP * CAP, D)
    expert_out = lax.map(expert, (expert_in, w_gate, w_up, w_down))
    by_block = expert_out.reshape(EXPERTS, N_EP, CAP, D).transpose(1, 0, 2, 3).reshape(N_EP, EXPERTS * CAP, D)
    block_ids = jnp.arange(N_EP, dtype=jnp.int32)[:, None, None]
    picked = by_block[block_ids, places].astype(jnp.float32)
    weights = route_weights.reshape(N_EP, TOK_DEV, TOP_K)
    combined = lax.optimization_barrier(jnp.sum(weights[:, :, :, None] * picked, axis=2)).reshape(TOKENS, D)
    inverse_out = lax.rsqrt(lax.optimization_barrier(jnp.mean(combined * combined, axis=1, keepdims=True)) + EPS)
    return (combined * inverse_out * final_gain[None, :]).astype(jnp.bfloat16)
```

```python
import functools

import jax
import jax.numpy as jnp
from jax import lax
from jax.experimental import pallas as pl
from jax.experimental.pallas import tpu as pltpu
from jax.sharding import PartitionSpec as P

TOP_K = 6


EPS = 1e-06
MESH = pl.DeviceIdType.MESH
META = None


def slot_table(route_rows, experts_all, capacity):
    flattened = route_rows.reshape(-1)
    matches = (flattened[:, None] == jnp.arange(experts_all, dtype=jnp.int32)[None, :]).astype(
        jnp.int32
    )
    earlier = jnp.cumsum(matches, axis=0) - matches
    slot_of = jnp.sum(earlier * matches, axis=1)
    return (flattened * capacity + slot_of).reshape(route_rows.shape)


def per_device(tokens, norm_gain, routes, route_weights, w_gate, w_up, w_down, final_gain):
    tok_count, features = tokens.shape
    ep_size = lax.axis_size("ep")
    exp_local = w_gate.shape[0]
    experts_all = exp_local * ep_size
    capacity = max(2, min(tok_count, 2 * tok_count * TOP_K // experts_all))
    slot_count = experts_all * capacity
    tokens_f = tokens.astype(jnp.float32)
    inverse = lax.rsqrt(jnp.mean(tokens_f * tokens_f, axis=1, keepdims=True) + EPS)
    normed = (tokens_f * inverse * norm_gain[None, :]).astype(jnp.bfloat16)
    places = slot_table(routes, experts_all, capacity)
    slot_ids = jnp.arange(slot_count, dtype=jnp.int32)
    matched = places[:, :, None] == slot_ids[None, None, :]
    selector = jnp.sum(matched.astype(jnp.float32), axis=1).T.astype(jnp.bfloat16)
    combine_rows = jnp.sum(jnp.where(matched, route_weights[:, :, None], 0.0), axis=1)
    outgoing = jnp.dot(selector, normed, preferred_element_type=jnp.float32).astype(jnp.bfloat16)
    outgoing = outgoing.reshape(ep_size, exp_local, capacity, features)
    received = lax.all_to_all(outgoing, "ep", split_axis=0, concat_axis=0, tiled=True)
    gate_value = jnp.einsum("secd,edf->secf", received, w_gate, preferred_element_type=jnp.float32)
    up_value = jnp.einsum("secd,edf->secf", received, w_up, preferred_element_type=jnp.float32)
    hidden = (jax.nn.silu(gate_value) * up_value).astype(jnp.bfloat16)
    partial_value = jnp.einsum("secf,efd->secd", hidden, w_down, preferred_element_type=jnp.float32)
    summed = lax.psum_scatter(
        partial_value.astype(jnp.bfloat16), "tp", scatter_dimension=3, tiled=True
    )
    returned = lax.all_to_all(summed, "ep", split_axis=0, concat_axis=0, tiled=True)
    results = returned.reshape(slot_count, returned.shape[3]).astype(jnp.float32)
    combined = jnp.dot(combine_rows, results, precision=lax.Precision.HIGHEST)
    local_squares = jnp.sum(combined * combined, axis=1)
    squares_all = lax.psum(local_squares, "tp")
    inverse_out = lax.rsqrt(squares_all / features + EPS)
    return (combined * inverse_out[:, None] * final_gain[None, :]).astype(jnp.bfloat16)


def fused_kernel(nz, tile, pieces, tokens_ref, gain_ref, routes_ref, rw_ref, wg_hbm, wu_hbm, wd_hbm, fgain_ref,
                 out_ref, buf, wg, wu, wd, hid, part, dbuf, xbuf, zbuf, total, meta, wsem,
                 az_s, az_r, ax_s, ax_r, ad_s, ad_r, md_s, md_r, rd_s, rd_r, rx_s, rx_r, rz_s, rz_r):
    rows, features = tokens_ref.shape
    hidden_units = wg.shape[1]
    experts = 4 * nz
    chunk = 4 * rows
    sub = rows // pieces
    halves, half = part.shape[1], part.shape[3]
    f32, bf16 = jnp.float32, jnp.bfloat16
    me = lax.axis_index("ep")
    core = lax.rem(me, 2)
    x = lax.rem(lax.div(me, 2), 2)
    z = lax.div(me, 4)
    d_peer = me + 1 - 2 * core
    x_peer = me + 2 - 4 * x
    has_below, has_above = z > 0, z < nz - 1
    inner = jnp.logical_and(has_below, has_above)
    outer = jnp.logical_not(inner)

    def weight_copy(which, j):
        src, dst = ((wg_hbm, wg), (wu_hbm, wu), (wd_hbm, wd))[which]
        cols = pl.ds(pl.multiple_of(j * tile, tile), tile)
        return pltpu.make_async_copy(src.at[0, :, cols], dst.at[:, cols], wsem.at[which, j])

    barrier = pltpu.get_barrier_semaphore()

    def greet(peer):
        pl.semaphore_signal(barrier, inc=1, device_id={"ep": peer}, device_id_type=MESH)

    greet(d_peer)
    greet(x_peer)
    pl.when(has_below)(lambda: greet(me - 4))
    pl.when(has_above)(lambda: greet(me + 4))

    gu_tiles, d_tiles = hidden_units // tile, features // tile
    for j in range(gu_tiles):
        weight_copy(0, j).start()
        weight_copy(1, j).start()
    for j in range(d_tiles):
        weight_copy(2, j).start()

    own = pl.ds(pl.multiple_of(me * rows, rows), rows)
    tok = tokens_ref[...].astype(f32)
    inverse = lax.rsqrt(jnp.mean(tok * tok, axis=1, keepdims=True) + EPS)
    buf[own, :] = (tok * inverse * gain_ref[...]).astype(bf16)
    lanes = lax.broadcasted_iota(jnp.int32, (experts, rows), 0)
    spread = jnp.zeros((experts, rows), f32)
    for k in range(routes_ref.shape[0]):
        spread = spread + jnp.where(lanes == routes_ref[k:k + 1, :], rw_ref[k:k + 1, :], 0.0)
    meta[me, :, :rows] = spread[:experts // 2]
    meta[me, :, rows:] = spread[experts // 2:]

    pl.semaphore_wait(barrier, jnp.where(inner, 4, 3))

    def remote(src, dst, s, r, dev):
        return pltpu.make_async_remote_copy(
            src_ref=src, dst_ref=dst, send_sem=s, recv_sem=r, device_id={"ep": dev}, device_id_type=MESH
        )

    own_step = nz - 1

    def order(q):
        rest = [p for p in range(nz) if p != q]
        if q in (0, nz - 1):
            return sorted(rest, key=lambda p: -abs(p - q))
        edge = 0 if 2 * q < nz else nz - 1
        return [edge] + sorted((p for p in rest if p != edge), key=lambda p: -abs(p - q))

    tables = [order(q) for q in range(nz)]
    places = []
    for i in range(own_step):
        value = tables[0][i]
        for q in range(1, nz):
            value = jnp.where(z == q, tables[q][i], value)
        places.append(value)
    places.append(z)

    def block_of(i, same_x, same_core):
        col = x if same_x else 1 - x
        lane = core if same_core else 1 - core
        return places[i] * 4 + col * 2 + lane

    def rows_of(i, same_x, same_core, q=None):
        at = block_of(i, same_x, same_core) * rows
        if q is None:
            return buf.at[pl.ds(pl.multiple_of(at, rows), rows), :]
        return buf.at[pl.ds(pl.multiple_of(at + q * sub, sub), sub), :]

    def piece(i, same_x, q):
        if q is META:
            return meta.at[block_of(i, same_x, True)]
        return rows_of(i, same_x, True, q)

    def slot_of(q):
        return pieces if q is META else q

    def ag_z(i, q, up):
        ref = piece(i, True, q)
        peer = me + 4 if up else me - 4
        return remote(ref, ref, az_s.at[i, int(up), slot_of(q)], az_r.at[places[i], slot_of(q)], peer)

    def ag_x(i, q, arriving=False):
        ref = piece(i, not arriving, q)
        return remote(ref, ref, ax_s.at[i, slot_of(q)], ax_r.at[i, slot_of(q)], x_peer)

    def ag_d(i, j, q):
        ref = piece(i, j == 0, q)
        s, r = (md_s, md_r) if q is META else (ad_s, ad_r)
        return remote(ref, ref, s.at[i, j], r.at[i, j], d_peer)

    def ag_d_all(i, j, arriving):
        ref = rows_of(i, j == 0, not arriving)
        return remote(ref, ref, ad_s.at[i, j], ad_r.at[i, j], d_peer)

    def meta_arrives(i, j):
        ref = meta.at[block_of(i, j == 0, False)]
        remote(ref, ref, md_s.at[i, j], md_r.at[i, j], d_peer).wait_recv()

    def start(copy):
        copy.start()

    def send_up(i, q, action):
        cond = has_above if i == own_step else jnp.logical_and(has_above, places[i] < z)
        pl.when(cond)(lambda: action(ag_z(i, q, True)))

    def send_down(i, q, action):
        cond = has_below if i == own_step else jnp.logical_and(has_below, places[i] > z)
        pl.when(cond)(lambda: action(ag_z(i, q, False)))

    def pass_on(i, q, action):
        send_up(i, q, action)
        send_down(i, q, action)

    def z_in(i, q):
        ag_z(i, q, True).wait_recv()
        pass_on(i, q, start)
        ag_d(i, 0, q).start()

    def x_out(i, q):
        ag_x(i, q).start()

    def x_in(i, q):
        ag_x(i, q, True).wait_recv()
        ag_d(i, 1, q).start()

    def rs_block(i, j, same_x, same_core):
        col = x if same_x else 1 - x
        lane = core if same_core else 1 - core
        at = pl.multiple_of((col * 2 + lane) * rows, rows)
        return part.at[i, j, pl.ds(at, rows), :]

    def rs_d(i, k, j):
        return remote(rs_block(i, j, k == 0, False), dbuf.at[i, k, j], rd_s.at[i, k, j], rd_r.at[i, k, j], d_peer)

    def rs_x(i, j):
        return remote(rs_block(i, j, False, True), xbuf.at[i, j], rx_s.at[i, j], rx_r.at[i, j], x_peer)

    def rs_z(i, j):
        up = places[i] > z
        slot = jnp.where(places[i] == z - 1, nz, places[i])
        peer = jnp.where(up, me + 4, me - 4)
        return remote(rs_block(i, j, True, True), zbuf.at[slot, j], rz_s.at[i, j], rz_r.at[slot, j], peer)

    def rs_z_arriving(slot, j):
        ref = zbuf.at[slot, j]
        return remote(ref, ref, rz_s.at[0, j], rz_r.at[slot, j], x_peer)

    def chunk_rows(i):
        return pl.ds(pl.multiple_of(places[i] * chunk, chunk), chunk)

    def gate_up(i, j):
        if i == own_step:
            weight_copy(0, j).wait()
            weight_copy(1, j).wait()
        cols = pl.ds(pl.multiple_of(j * tile, tile), tile)
        lhs = buf[chunk_rows(i), :]
        g = jnp.dot(lhs, wg[:, cols], preferred_element_type=f32)
        u = jnp.dot(lhs, wu[:, cols], preferred_element_type=f32)
        hid[:, cols] = (g / (1.0 + jnp.exp(-g)) * u).astype(bf16)

    def weight_of(i):
        eye = lax.broadcasted_iota(jnp.int32, (rows, rows), 0) == lax.broadcasted_iota(jnp.int32, (rows, rows), 1)
        line, side = lax.rem(me, experts // 2), lax.div(me, experts // 2)
        cols = []
        for b in range(4):
            both = meta[places[i] * 4 + b, pl.ds(line, 1), :]
            row = jnp.where(side == 0, both[:, :rows], both[:, rows:])
            cols.append(jnp.sum(jnp.where(eye, row, 0.0), axis=1, keepdims=True))
        return jnp.concatenate(cols, axis=0)

    def down(i):
        weight = weight_of(i)
        per = half // tile
        for j in range(halves):
            def body(t, carry):
                if i == own_step:
                    weight_copy(2, j * per + t).wait()
                cols = pl.ds(pl.multiple_of((j * per + t) * tile, tile), tile)
                o = jnp.dot(hid[...], wd[:, cols], preferred_element_type=f32)
                part[i, j, :, pl.ds(pl.multiple_of(t * tile, tile), tile)] = (o * weight).astype(bf16)
                return carry

            lax.fori_loop(0, per, body, 0)
            rs_d(i, 1, j).start()
            rs_d(i, 0, j).start()

    def finish_d(i, j):
        rs_d(i, 1, j).wait_recv()
        ref = rs_block(i, j, False, True)
        ref[...] = (ref[...].astype(f32) + dbuf[i, 1, j].astype(f32)).astype(bf16)
        rs_x(i, j).start()

    def finish_x(i, j):
        rs_d(i, 0, j).wait_recv()
        rs_x(i, j).wait_recv()
        ref = rs_block(i, j, True, True)
        value = ref[...].astype(f32) + dbuf[i, 0, j].astype(f32) + xbuf[i, j].astype(f32)
        if i == own_step:
            total[j] = value
        else:
            ref[...] = value.astype(bf16)
            pl.when(outer)(lambda: rs_z(i, j).start())

    def merge(i, j):
        rs_z_arriving(places[i], j).wait_recv()
        ref = rs_block(i, j, True, True)
        ref[...] = (ref[...].astype(f32) + zbuf[places[i], j].astype(f32)).astype(bf16)
        rs_z(i, j).start()

    def loop(i, duties):
        def body(j, carry):
            gate_up(i, j)
            duties(j)
            return carry

        lax.fori_loop(0, gu_tiles, body, 0)

    first = pieces // 2
    pass_on(own_step, META, start)
    x_out(own_step, META)
    ag_d(own_step, 0, META).start()
    for q in range(pieces):
        x_out(own_step, q)
        if q < first:
            pass_on(own_step, q, start)
        else:
            pl.when(outer)(lambda: pass_on(own_step, q, start))
        ag_d(own_step, 0, q).start()

    def late_inward(q):
        pl.when(2 * z < nz)(lambda: send_up(own_step, q, start))
        pl.when(2 * z >= nz)(lambda: send_down(own_step, q, start))

    def late_outward(q):
        pl.when(2 * z < nz)(lambda: send_down(own_step, q, start))
        pl.when(2 * z >= nz)(lambda: send_up(own_step, q, start))

    for q in range(first):
        x_in(own_step, q)

        @pl.when(inner)
        def _():
            z_in(0, q)
            x_out(0, q)
            z_in(2, q)

        @pl.when(outer)
        def _():
            z_in(2, q)
            x_out(2, q)

    for q in range(first, pieces):
        x_in(own_step, q)

        @pl.when(inner)
        def _():
            z_in(0, q)
            x_out(0, q)
            z_in(1, q - first)

        @pl.when(outer)
        def _():
            z_in(1, q - first)

    @pl.when(inner)
    def _():
        for q in range(first, pieces):
            late_inward(q)
        for q in range(first):
            x_out(1, q)
        z_in(0, META)
        x_out(0, META)

    x_in(own_step, META)
    z_in(2, META)
    x_out(2, META)
    ag_d_all(own_step, 0, True).wait_recv()
    ag_d_all(own_step, 1, True).wait_recv()

    def second_part(i, j):
        @pl.when(j < first)
        def _():
            z_in(i, j + first)
            x_out(i, j + first)

        @pl.when(j >= first)
        def _():
            z_in(2, j)

    def own_duties(j):
        @pl.when(inner)
        def _():
            second_part(1, j)

            @pl.when(j == first - 1)
            def _():
                for q in range(first, pieces):
                    late_outward(q)

        @pl.when(outer)
        def _():
            z_in(0, j)
            x_out(0, j)

        @pl.when(j >= 1)
        def _():
            x_in(0, j - 1)

    loop(own_step, own_duties)

    z_in(1, META)
    x_out(1, META)

    @pl.when(inner)
    def _():
        for q in range(pieces):
            x_out(2, q)

    @pl.when(outer)
    def _():
        for q in range(first):
            x_out(1, q)
        z_in(0, META)
        x_out(0, META)

    for j in range(2):
        meta_arrives(own_step, j)
    down(own_step)
    x_in(0, pieces - 1)
    for j in range(2):
        ag_d_all(0, j, True).wait_recv()

    def duties_0(j):
        @pl.when(outer)
        def _():
            second_part(1, j)
            pl.when(j >= first)(lambda: x_out(2, j))

        x_in(1, j)

    loop(0, duties_0)
    finish_d(own_step, 0)
    for i in range(own_step):
        x_in(i, META)
    for i in range(own_step):
        for j in range(2):
            meta_arrives(i, j)
    down(0)
    for j in range(2):
        ag_d_all(1, j, True).wait_recv()

    def duties_1(j):
        x_in(2, j)
        pl.when(j < halves)(lambda: finish_d(0, j))

    loop(1, duties_1)
    finish_x(own_step, 0)
    down(1)
    for j in range(2):
        ag_d_all(2, j, True).wait_recv()

    def duties_2(j):
        @pl.when(j < halves)
        def _():
            finish_d(1, j)
            finish_x(0, j)

    loop(2, duties_2)
    down(2)
    for j in range(halves):
        finish_d(2, j)
    finish_d(own_step, 1)
    for j in range(halves):
        finish_x(1, j)
        pl.when(inner)(lambda: merge(1, j))
    for j in range(halves):
        pl.when(inner)(lambda: merge(0, j))
    for j in range(halves):
        finish_x(2, j)
        pl.when(inner)(lambda: merge(2, j))
    finish_x(own_step, 1)

    @pl.when(has_below)
    def _():
        for j in range(halves):
            rs_z_arriving(z, j).wait_recv()
            total[j] = total[j] + zbuf[z, j].astype(f32)

    @pl.when(has_above)
    def _():
        for j in range(halves):
            rs_z_arriving(nz, j).wait_recv()
            total[j] = total[j] + zbuf[nz, j].astype(f32)

    squares = 0.0
    for j in range(halves):
        squares = squares + jnp.sum(total[j] * total[j], axis=1, keepdims=True)
    inverse_out = lax.rsqrt(squares / features + EPS)
    for j in range(halves):
        cols = pl.ds(j * half, half)
        out_ref[:, cols] = (total[j] * inverse_out * fgain_ref[:, cols]).astype(out_ref.dtype)

    for i in range(nz):
        for q in [META] + list(range(pieces)):
            pass_on(i, q, lambda copy: copy.wait_send())
            ag_x(i, q).wait_send()
        for j in range(2):
            ag_d(i, j, META).wait_send()
            ag_d_all(i, j, False).wait_send()
        for j in range(halves):
            rs_x(i, j).wait_send()
            for k in range(2):
                rs_d(i, k, j).wait_send()
            if i < own_step:
                rs_z(i, j).wait_send()


def fused_device(tokens, norm_gain, routes, route_weights, w_gate, w_up, w_down, final_gain):
    rows, features = tokens.shape
    hidden_units = w_gate.shape[2]
    experts = lax.axis_size("ep")
    nz = experts // 4
    pieces, halves = 4, 2
    tile = hidden_units // pieces
    half = features // halves
    vmem, anywhere = pl.BlockSpec(memory_space=pltpu.VMEM), pl.BlockSpec(memory_space=pl.ANY)
    dma = pltpu.SemaphoreType.DMA
    bf16 = jnp.bfloat16
    return pl.pallas_call(
        functools.partial(fused_kernel, nz, tile, pieces),
        out_shape=jax.ShapeDtypeStruct((rows, features), jnp.bfloat16),
        in_specs=[vmem, vmem, vmem, vmem, anywhere, anywhere, anywhere, vmem],
        out_specs=vmem,
        scratch_shapes=[
            pltpu.VMEM((experts * rows, features), bf16),
            pltpu.VMEM((features, hidden_units), bf16),
            pltpu.VMEM((features, hidden_units), bf16),
            pltpu.VMEM((hidden_units, features), bf16),
            pltpu.VMEM((4 * rows, hidden_units), bf16),
            pltpu.VMEM((nz, halves, 4 * rows, half), bf16),
            pltpu.VMEM((nz, 2, halves, rows, half), bf16),
            pltpu.VMEM((nz, halves, rows, half), bf16),
            pltpu.VMEM((nz + 1, halves, rows, half), bf16),
            pltpu.VMEM((halves, rows, half), jnp.float32),
            pltpu.VMEM((experts, experts // 2, 2 * rows), jnp.float32),
            dma((3, max(hidden_units, features) // tile)),
            dma((nz, 2, pieces + 1)), dma((nz, pieces + 1)), dma((nz, pieces + 1)), dma((nz, pieces + 1)),
            dma((nz, 2)), dma((nz, 2)), dma((nz, 2)), dma((nz, 2)),
            dma((nz, 2, halves)), dma((nz, 2, halves)), dma((nz, halves)), dma((nz, halves)),
            dma((nz, halves)), dma((nz + 1, halves)),
        ],
        compiler_params=pltpu.CompilerParams(
            collective_id=0, has_side_effects=True, vmem_limit_bytes=60 * 1024 * 1024
        ),
    )(tokens, norm_gain[None, :], routes.T, route_weights.T, w_gate, w_up, w_down, final_gain[None, :])


def solution(mesh):
    placed = (
        P(("grp", "ep"), None),
        P(),
        P(("grp", "ep"), None),
        P(("grp", "ep"), None),
        P("ep", None, "tp"),
        P("ep", None, "tp"),
        P("ep", "tp", None),
        P("tp"),
    )
    ep, tp = mesh.shape["ep"], mesh.shape["tp"]

    def step(*args):
        rows, features = args[0].shape
        hidden_units = args[4].shape[2]
        fits = 3 * features * hidden_units + 3 * ep * rows * features < 24 * 2 ** 20
        whole_tiles = features % 2048 == 0 and hidden_units % 2048 == 0 and rows % 64 == 0
        if tp == 1 and ep == 16 and args[4].shape[0] == 1 and fits and whole_tiles:
            return fused_device(*args)
        return per_device(*args)

    return jax.shard_map(
        step, mesh=mesh, in_specs=placed, out_specs=P(("grp", "ep"), "tp"), check_vma=False
    )
```

```python
import functools

import jax
import jax.numpy as jnp
from jax import lax
from jax.experimental import pallas as pl
from jax.experimental.pallas import tpu as pltpu
from jax.sharding import PartitionSpec as P

TOP_K = 6


EPS = 1e-06
MESH = pl.DeviceIdType.MESH
META = None


def slot_table(route_rows, experts_all, capacity):
    flattened = route_rows.reshape(-1)
    matches = (flattened[:, None] == jnp.arange(experts_all, dtype=jnp.int32)[None, :]).astype(
        jnp.int32
    )
    earlier = jnp.cumsum(matches, axis=0) - matches
    slot_of = jnp.sum(earlier * matches, axis=1)
    return (flattened * capacity + slot_of).reshape(route_rows.shape)


def per_device(tokens, norm_gain, routes, route_weights, w_gate, w_up, w_down, final_gain):
    tok_count, features = tokens.shape
    ep_size = lax.axis_size("ep")
    exp_local = w_gate.shape[0]
    experts_all = exp_local * ep_size
    capacity = max(2, min(tok_count, 2 * tok_count * TOP_K // experts_all))
    slot_count = experts_all * capacity
    tokens_f = tokens.astype(jnp.float32)
    inverse = lax.rsqrt(jnp.mean(tokens_f * tokens_f, axis=1, keepdims=True) + EPS)
    normed = (tokens_f * inverse * norm_gain[None, :]).astype(jnp.bfloat16)
    places = slot_table(routes, experts_all, capacity)
    slot_ids = jnp.arange(slot_count, dtype=jnp.int32)
    matched = places[:, :, None] == slot_ids[None, None, :]
    selector = jnp.sum(matched.astype(jnp.float32), axis=1).T.astype(jnp.bfloat16)
    combine_rows = jnp.sum(jnp.where(matched, route_weights[:, :, None], 0.0), axis=1)
    outgoing = jnp.dot(selector, normed, preferred_element_type=jnp.float32).astype(jnp.bfloat16)
    outgoing = outgoing.reshape(ep_size, exp_local, capacity, features)
    received = lax.all_to_all(outgoing, "ep", split_axis=0, concat_axis=0, tiled=True)
    gate_value = jnp.einsum("secd,edf->secf", received, w_gate, preferred_element_type=jnp.float32)
    up_value = jnp.einsum("secd,edf->secf", received, w_up, preferred_element_type=jnp.float32)
    hidden = (jax.nn.silu(gate_value) * up_value).astype(jnp.bfloat16)
    partial_value = jnp.einsum("secf,efd->secd", hidden, w_down, preferred_element_type=jnp.float32)
    summed = lax.psum_scatter(
        partial_value.astype(jnp.bfloat16), "tp", scatter_dimension=3, tiled=True
    )
    returned = lax.all_to_all(summed, "ep", split_axis=0, concat_axis=0, tiled=True)
    results = returned.reshape(slot_count, returned.shape[3]).astype(jnp.float32)
    combined = jnp.dot(combine_rows, results, precision=lax.Precision.HIGHEST)
    local_squares = jnp.sum(combined * combined, axis=1)
    squares_all = lax.psum(local_squares, "tp")
    inverse_out = lax.rsqrt(squares_all / features + EPS)
    return (combined * inverse_out[:, None] * final_gain[None, :]).astype(jnp.bfloat16)


def fused_kernel(nz, tile, pieces, tokens_ref, gain_ref, routes_ref, rw_ref, wg_hbm, wu_hbm, wd_hbm, fgain_ref,
                 out_ref, buf, wg, wu, wd, hid, hid_own, part, dbuf, xbuf, zbuf, total, meta, wsem,
                 az_s, az_r, ax_s, ax_r, ad_s, ad_r, md_s, md_r, rd_s, rd_r, rx_s, rx_r, rz_s, rz_r):
    rows, features = tokens_ref.shape
    hidden_units = wg.shape[1]
    experts = 4 * nz
    chunk = 4 * rows
    sub = rows // pieces
    halves, half = part.shape[1], part.shape[3]
    f32, bf16 = jnp.float32, jnp.bfloat16
    me = lax.axis_index("ep")
    core = lax.rem(me, 2)
    x = lax.rem(lax.div(me, 2), 2)
    z = lax.div(me, 4)
    d_peer = me + 1 - 2 * core
    x_peer = me + 2 - 4 * x
    has_below, has_above = z > 0, z < nz - 1
    inner = jnp.logical_and(has_below, has_above)
    outer = jnp.logical_not(inner)

    def weight_copy(which, j):
        src, dst = ((wg_hbm, wg), (wu_hbm, wu), (wd_hbm, wd))[which]
        cols = pl.ds(pl.multiple_of(j * tile, tile), tile)
        return pltpu.make_async_copy(src.at[0, :, cols], dst.at[:, cols], wsem.at[which, j])

    barrier = pltpu.get_barrier_semaphore()

    def greet(peer):
        pl.semaphore_signal(barrier, inc=1, device_id={"ep": peer}, device_id_type=MESH)

    greet(d_peer)
    greet(x_peer)
    pl.when(has_below)(lambda: greet(me - 4))
    pl.when(has_above)(lambda: greet(me + 4))

    gu_tiles, d_tiles = hidden_units // tile, features // tile
    for j in range(gu_tiles):
        weight_copy(0, j).start()
        weight_copy(1, j).start()
    for j in range(d_tiles):
        weight_copy(2, j).start()

    own = pl.ds(pl.multiple_of(me * rows, rows), rows)
    tok = tokens_ref[...].astype(f32)
    inverse = lax.rsqrt(jnp.mean(tok * tok, axis=1, keepdims=True) + EPS)
    buf[own, :] = (tok * inverse * gain_ref[...]).astype(bf16)
    lanes = lax.broadcasted_iota(jnp.int32, (experts, rows), 0)
    spread = jnp.zeros((experts, rows), f32)
    for k in range(routes_ref.shape[0]):
        spread = spread + jnp.where(lanes == routes_ref[k:k + 1, :], rw_ref[k:k + 1, :], 0.0)
    meta[me, :, :rows] = spread[:experts // 2]
    meta[me, :, rows:] = spread[experts // 2:]

    pl.semaphore_wait(barrier, jnp.where(inner, 4, 3))

    def remote(src, dst, s, r, dev):
        return pltpu.make_async_remote_copy(
            src_ref=src, dst_ref=dst, send_sem=s, recv_sem=r, device_id={"ep": dev}, device_id_type=MESH
        )

    own_step = nz - 1

    def order(q):
        edge = 0 if 2 * q < nz else nz - 1
        far = nz - 1 - edge
        if q == edge:
            near = q + 1 if q == 0 else q - 1
            return [near, far] + [p for p in range(nz) if p not in (q, near, far)]
        return [p for p in range(nz) if p not in (q, edge, far)] + [far, edge]

    tables = [order(q) for q in range(nz)]
    places = []
    for i in range(own_step):
        value = tables[0][i]
        for q in range(1, nz):
            value = jnp.where(z == q, tables[q][i], value)
        places.append(value)
    places.append(z)

    def block_of(i, same_x, same_core):
        col = x if same_x else 1 - x
        lane = core if same_core else 1 - core
        return places[i] * 4 + col * 2 + lane

    def rows_of(i, same_x, same_core, q=None):
        at = block_of(i, same_x, same_core) * rows
        if q is None:
            return buf.at[pl.ds(pl.multiple_of(at, rows), rows), :]
        return buf.at[pl.ds(pl.multiple_of(at + q * sub, sub), sub), :]

    def piece(i, same_x, q):
        if q is META:
            return meta.at[block_of(i, same_x, True)]
        return rows_of(i, same_x, True, q)

    def slot_of(q):
        return pieces if q is META else q

    def ag_z(i, q, up):
        ref = piece(i, True, q)
        peer = me + 4 if up else me - 4
        return remote(ref, ref, az_s.at[i, int(up), slot_of(q)], az_r.at[places[i], slot_of(q)], peer)

    def ag_x(i, q, arriving=False):
        ref = piece(i, not arriving, q)
        return remote(ref, ref, ax_s.at[i, slot_of(q)], ax_r.at[i, slot_of(q)], x_peer)

    def ag_d(i, j, q):
        ref = piece(i, j == 0, q)
        s, r = (md_s, md_r) if q is META else (ad_s, ad_r)
        return remote(ref, ref, s.at[i, j], r.at[i, j], d_peer)

    def ag_d_all(i, j, arriving):
        ref = rows_of(i, j == 0, not arriving)
        return remote(ref, ref, ad_s.at[i, j], ad_r.at[i, j], d_peer)

    def meta_arrives(i, j):
        ref = meta.at[block_of(i, j == 0, False)]
        remote(ref, ref, md_s.at[i, j], md_r.at[i, j], d_peer).wait_recv()

    def start(copy):
        copy.start()

    def send_up(i, q, action):
        cond = has_above if i == own_step else jnp.logical_and(has_above, places[i] < z)
        pl.when(cond)(lambda: action(ag_z(i, q, True)))

    def send_down(i, q, action):
        cond = has_below if i == own_step else jnp.logical_and(has_below, places[i] > z)
        pl.when(cond)(lambda: action(ag_z(i, q, False)))

    def pass_on(i, q, action):
        send_up(i, q, action)
        send_down(i, q, action)

    def z_in(i, q):
        ag_z(i, q, True).wait_recv()
        pass_on(i, q, start)
        ag_d(i, 0, q).start()

    def x_out(i, q):
        ag_x(i, q).start()

    def x_in(i, q):
        ag_x(i, q, True).wait_recv()
        ag_d(i, 1, q).start()

    def rs_block(i, j, same_x, same_core):
        col = x if same_x else 1 - x
        lane = core if same_core else 1 - core
        at = pl.multiple_of((col * 2 + lane) * rows, rows)
        return part.at[i, j, pl.ds(at, rows), :]

    def rs_d(i, k, j):
        return remote(rs_block(i, j, k == 0, False), dbuf.at[i, k, j], rd_s.at[i, k, j], rd_r.at[i, k, j], d_peer)

    def rs_x(i, j):
        return remote(rs_block(i, j, False, True), xbuf.at[i, j], rx_s.at[i, j], rx_r.at[i, j], x_peer)

    def rs_z(i, j):
        level, slot = places[i], z
        if i == 1:
            level = jnp.where(outer, jnp.where(has_below, z - 1, z + 1), level)
            slot = jnp.where(outer, nz, slot)
        peer = level * 4 + x * 2 + core
        return remote(rs_block(i, j, True, True), zbuf.at[slot, j], rz_s.at[i, j], rz_r.at[slot, j], peer)

    def rs_z_arriving(slot, j):
        ref = zbuf.at[slot, j]
        return remote(ref, ref, rz_s.at[0, j], rz_r.at[slot, j], x_peer)

    def chunk_rows(i):
        return pl.ds(pl.multiple_of(places[i] * chunk, chunk), chunk)

    def gate_up_rows(source, kept, target, j):
        cols = pl.ds(pl.multiple_of(j * tile, tile), tile)
        lhs = buf[source, :]
        g = jnp.dot(lhs, wg[:, cols], preferred_element_type=f32)
        u = jnp.dot(lhs, wu[:, cols], preferred_element_type=f32)
        kept[target, cols] = (g / (1.0 + jnp.exp(-g)) * u).astype(bf16)

    def gate_up(i, j):
        gate_up_rows(chunk_rows(i), hid, pl.ds(0, chunk), j)

    def gate_up_chip(j, col, fresh):
        if fresh:
            weight_copy(0, j).wait()
            weight_copy(1, j).wait()
        at = pl.multiple_of(col * (2 * rows), 2 * rows)
        start_row = pl.multiple_of(z * chunk + col * (2 * rows), 2 * rows)
        gate_up_rows(pl.ds(start_row, 2 * rows), hid_own, pl.ds(at, 2 * rows), j)

    def weight_of(i):
        eye = lax.broadcasted_iota(jnp.int32, (rows, rows), 0) == lax.broadcasted_iota(jnp.int32, (rows, rows), 1)
        line, side = lax.rem(me, experts // 2), lax.div(me, experts // 2)
        cols = []
        for b in range(4):
            both = meta[places[i] * 4 + b, pl.ds(line, 1), :]
            row = jnp.where(side == 0, both[:, :rows], both[:, rows:])
            cols.append(jnp.sum(jnp.where(eye, row, 0.0), axis=1, keepdims=True))
        return jnp.concatenate(cols, axis=0)

    def down(i, duties):
        weight = weight_of(i)
        kept = hid_own if i == own_step else hid

        def body(t, carry):
            if i == 0:
                weight_copy(2, t).wait()
            cols = pl.ds(pl.multiple_of(t * tile, tile), tile)
            o = jnp.dot(kept[...], wd[:, cols], preferred_element_type=f32)
            part[i, t] = (o * weight).astype(bf16)
            rs_d(i, 1, t).start()
            rs_d(i, 0, t).start()
            duties(t)
            return carry

        lax.fori_loop(0, d_tiles, body, 0)

    def finish_d(i, j):
        rs_d(i, 1, j).wait_recv()
        ref = rs_block(i, j, False, True)
        ref[...] = (ref[...].astype(f32) + dbuf[i, 1, j].astype(f32)).astype(bf16)
        rs_x(i, j).start()

    def finish_x(i, j):
        rs_d(i, 0, j).wait_recv()
        rs_x(i, j).wait_recv()
        ref = rs_block(i, j, True, True)
        value = ref[...].astype(f32) + dbuf[i, 0, j].astype(f32) + xbuf[i, j].astype(f32)
        if i == own_step:
            total[j] = value
        else:
            ref[...] = value.astype(bf16)
            if i == 1:
                @pl.when(inner)
                def _():
                    rs_z_arriving(nz, j).wait_recv()
                    ref[...] = (value + zbuf[nz, j].astype(f32)).astype(bf16)
            rs_z(i, j).start()

    def loop(i, duties):
        def body(j, carry):
            gate_up(i, j)
            duties(j)
            return carry

        lax.fori_loop(0, gu_tiles, body, 0)

    def chunk_ready(i):
        for j in range(2):
            ag_d_all(i, j, True).wait_recv()

    def step(body):
        lax.fori_loop(0, pieces, lambda j, carry: (body(j), carry)[1], 0)

    for q in [META] + list(range(pieces)):
        x_out(own_step, q)
        pass_on(own_step, q, start)
        ag_d(own_step, 0, q).start()

    z_in(0, META)
    x_out(0, META)

    @pl.when(inner)
    def _():
        z_in(2, META)
        x_out(2, META)

    ag_d_all(own_step, 0, True).wait_recv()

    def gather(q):
        gate_up_chip(q, x, True)
        x_in(own_step, q)
        z_in(0, q)
        x_out(0, q)
        pl.when(inner)(lambda: z_in(2, q))

    step(gather)

    @pl.when(inner)
    def _():
        z_in(1, META)
        x_out(1, META)

    @pl.when(outer)
    def _():
        z_in(2, META)
        x_out(2, META)

    ag_d_all(own_step, 1, True).wait_recv()

    def own_rest(j):
        gate_up_chip(j, 1 - x, False)

        @pl.when(inner)
        def _():
            z_in(1, j)
            x_out(1, j)

        @pl.when(outer)
        def _():
            z_in(2, j)
            x_out(2, j)

        x_in(0, j)

    step(own_rest)

    @pl.when(inner)
    def _():
        for q in range(pieces):
            x_out(2, q)

    x_in(own_step, META)
    x_in(0, META)
    chunk_ready(0)

    def far_in(q):
        z_in(1, q)
        x_out(1, q)

    def duties_0(j):
        pl.when(outer)(lambda: far_in(j))
        pl.when(inner)(lambda: x_in(1, j))

    loop(0, duties_0)

    @pl.when(outer)
    def _():
        z_in(1, META)
        x_out(1, META)

    for j in range(2):
        meta_arrives(0, j)

    def down_duties_0(t):
        pl.when(t >= 2)(lambda: finish_d(0, t - 2))
        pl.when(outer)(lambda: x_in(1, t))

    down(0, down_duties_0)
    x_in(1, META)
    x_in(2, META)
    chunk_ready(1)

    def duties_1(j):
        pl.when(j < 2)(lambda: finish_d(0, j + 2))
        x_in(2, j)
        pl.when(j >= 2)(lambda: finish_x(0, j - 2))

    loop(1, duties_1)
    for i in range(1, nz):
        for j in range(2):
            meta_arrives(i, j)

    def down_duties_1(t):
        @pl.when(t >= 2)
        def _():
            finish_d(1, t - 2)
            finish_x(0, t)

    down(1, down_duties_1)
    chunk_ready(2)

    def duties_2(j):
        pl.when(j < 2)(lambda: finish_d(1, j + 2))
        pl.when(jnp.logical_and(j >= 2, outer))(lambda: finish_x(1, j - 2))

    loop(2, duties_2)

    def down_duties_2(t):
        pl.when(t >= 2)(lambda: finish_d(2, t - 2))
        pl.when(jnp.logical_and(t < 2, outer))(lambda: finish_x(1, t + 2))

    down(2, down_duties_2)

    def down_duties_own(t):
        pl.when(t < 2)(lambda: finish_d(2, t + 2))
        pl.when(t >= 2)(lambda: finish_d(own_step, t - 2))
        pl.when(inner)(lambda: finish_x(1, t))

    down(own_step, down_duties_own)
    finish_x(2, 0)
    finish_d(own_step, 2)
    finish_x(2, 1)
    finish_d(own_step, 3)
    finish_x(2, 2)
    finish_x(2, 3)
    for i in range(nz):
        for q in [META] + list(range(pieces)):
            pass_on(i, q, lambda copy: copy.wait_send())
            ag_x(i, q).wait_send()
        for j in range(2):
            ag_d(i, j, META).wait_send()
            ag_d_all(i, j, False).wait_send()
    step(lambda j: finish_x(own_step, j))

    def collect(level, cond):
        def one(j):
            rs_z_arriving(level, j).wait_recv()
            total[j] = total[j] + zbuf[level, j].astype(f32)

        pl.when(cond)(lambda: step(one))

    for level in range(nz):
        cond = z != level
        if level in (0, nz - 1):
            cond = jnp.logical_and(cond, inner)
        collect(level, cond)

    squares = 0.0
    for j in range(halves):
        squares = squares + jnp.sum(total[j] * total[j], axis=1, keepdims=True)
    inverse_out = lax.rsqrt(squares / features + EPS)
    for j in range(halves):
        cols = pl.ds(j * half, half)
        out_ref[:, cols] = (total[j] * inverse_out * fgain_ref[:, cols]).astype(out_ref.dtype)

    for i in range(nz):
        for j in range(halves):
            rs_x(i, j).wait_send()
            for k in range(2):
                rs_d(i, k, j).wait_send()
            if i < own_step:
                rs_z(i, j).wait_send()


def fused_device(tokens, norm_gain, routes, route_weights, w_gate, w_up, w_down, final_gain):
    rows, features = tokens.shape
    hidden_units = w_gate.shape[2]
    experts = lax.axis_size("ep")
    nz = experts // 4
    pieces, halves = 4, 4
    tile = hidden_units // pieces
    half = features // halves
    vmem, anywhere = pl.BlockSpec(memory_space=pltpu.VMEM), pl.BlockSpec(memory_space=pl.ANY)
    dma = pltpu.SemaphoreType.DMA
    bf16 = jnp.bfloat16
    return pl.pallas_call(
        functools.partial(fused_kernel, nz, tile, pieces),
        out_shape=jax.ShapeDtypeStruct((rows, features), jnp.bfloat16),
        in_specs=[vmem, vmem, vmem, vmem, anywhere, anywhere, anywhere, vmem],
        out_specs=vmem,
        scratch_shapes=[
            pltpu.VMEM((experts * rows, features), bf16),
            pltpu.VMEM((features, hidden_units), bf16),
            pltpu.VMEM((features, hidden_units), bf16),
            pltpu.VMEM((hidden_units, features), bf16),
            pltpu.VMEM((4 * rows, hidden_units), bf16),
            pltpu.VMEM((4 * rows, hidden_units), bf16),
            pltpu.VMEM((nz, halves, 4 * rows, half), bf16),
            pltpu.VMEM((nz, 2, halves, rows, half), bf16),
            pltpu.VMEM((nz, halves, rows, half), bf16),
            pltpu.VMEM((nz + 1, halves, rows, half), bf16),
            pltpu.VMEM((halves, rows, half), jnp.float32),
            pltpu.VMEM((experts, experts // 2, 2 * rows), jnp.float32),
            dma((3, max(hidden_units, features) // tile)),
            dma((nz, 2, pieces + 1)), dma((nz, pieces + 1)), dma((nz, pieces + 1)), dma((nz, pieces + 1)),
            dma((nz, 2)), dma((nz, 2)), dma((nz, 2)), dma((nz, 2)),
            dma((nz, 2, halves)), dma((nz, 2, halves)), dma((nz, halves)), dma((nz, halves)),
            dma((nz, halves)), dma((nz + 1, halves)),
        ],
        compiler_params=pltpu.CompilerParams(
            collective_id=0, has_side_effects=True, vmem_limit_bytes=60 * 1024 * 1024
        ),
    )(tokens, norm_gain[None, :], routes.T, route_weights.T, w_gate, w_up, w_down, final_gain[None, :])


def solution(mesh):
    placed = (
        P(("grp", "ep"), None),
        P(),
        P(("grp", "ep"), None),
        P(("grp", "ep"), None),
        P("ep", None, "tp"),
        P("ep", None, "tp"),
        P("ep", "tp", None),
        P("tp"),
    )
    ep, tp = mesh.shape["ep"], mesh.shape["tp"]

    def step(*args):
        rows, features = args[0].shape
        hidden_units = args[4].shape[2]
        fits = 3 * features * hidden_units + 3 * ep * rows * features < 24 * 2 ** 20
        whole_tiles = features % 2048 == 0 and hidden_units % 2048 == 0 and rows % 64 == 0
        if tp == 1 and ep == 16 and args[4].shape[0] == 1 and fits and whole_tiles:
            return fused_device(*args)
        return per_device(*args)

    return jax.shard_map(
        step, mesh=mesh, in_specs=placed, out_specs=P(("grp", "ep"), "tp"), check_vma=False
    )
```

```python
import functools

import jax
import jax.numpy as jnp
from jax import lax
from jax.experimental import pallas as pl
from jax.experimental.pallas import tpu as pltpu
from jax.sharding import PartitionSpec as P

TOP_K = 6


EPS = 1e-06
MESH = pl.DeviceIdType.MESH
META = None


def slot_table(route_rows, experts_all, capacity):
    flattened = route_rows.reshape(-1)
    matches = (flattened[:, None] == jnp.arange(experts_all, dtype=jnp.int32)[None, :]).astype(
        jnp.int32
    )
    earlier = jnp.cumsum(matches, axis=0) - matches
    slot_of = jnp.sum(earlier * matches, axis=1)
    return (flattened * capacity + slot_of).reshape(route_rows.shape)


def per_device(tokens, norm_gain, routes, route_weights, w_gate, w_up, w_down, final_gain):
    tok_count, features = tokens.shape
    ep_size = lax.axis_size("ep")
    exp_local = w_gate.shape[0]
    experts_all = exp_local * ep_size
    capacity = max(2, min(tok_count, 2 * tok_count * TOP_K // experts_all))
    slot_count = experts_all * capacity
    tokens_f = tokens.astype(jnp.float32)
    inverse = lax.rsqrt(jnp.mean(tokens_f * tokens_f, axis=1, keepdims=True) + EPS)
    normed = (tokens_f * inverse * norm_gain[None, :]).astype(jnp.bfloat16)
    places = slot_table(routes, experts_all, capacity)
    slot_ids = jnp.arange(slot_count, dtype=jnp.int32)
    matched = places[:, :, None] == slot_ids[None, None, :]
    selector = jnp.sum(matched.astype(jnp.float32), axis=1).T.astype(jnp.bfloat16)
    combine_rows = jnp.sum(jnp.where(matched, route_weights[:, :, None], 0.0), axis=1)
    outgoing = jnp.dot(selector, normed, preferred_element_type=jnp.float32).astype(jnp.bfloat16)
    outgoing = outgoing.reshape(ep_size, exp_local, capacity, features)
    received = lax.all_to_all(outgoing, "ep", split_axis=0, concat_axis=0, tiled=True)
    gate_value = jnp.einsum("secd,edf->secf", received, w_gate, preferred_element_type=jnp.float32)
    up_value = jnp.einsum("secd,edf->secf", received, w_up, preferred_element_type=jnp.float32)
    hidden = (jax.nn.silu(gate_value) * up_value).astype(jnp.bfloat16)
    partial_value = jnp.einsum("secf,efd->secd", hidden, w_down, preferred_element_type=jnp.float32)
    summed = lax.psum_scatter(
        partial_value.astype(jnp.bfloat16), "tp", scatter_dimension=3, tiled=True
    )
    returned = lax.all_to_all(summed, "ep", split_axis=0, concat_axis=0, tiled=True)
    results = returned.reshape(slot_count, returned.shape[3]).astype(jnp.float32)
    combined = jnp.dot(combine_rows, results, precision=lax.Precision.HIGHEST)
    local_squares = jnp.sum(combined * combined, axis=1)
    squares_all = lax.psum(local_squares, "tp")
    inverse_out = lax.rsqrt(squares_all / features + EPS)
    return (combined * inverse_out[:, None] * final_gain[None, :]).astype(jnp.bfloat16)


def fused_kernel(nz, tile, pieces, tokens_ref, gain_ref, routes_ref, rw_ref, wg_hbm, wu_hbm, wd_hbm, fgain_ref,
                 out_ref, buf, wg, wu, wd, hid, hid_own, part, dbuf, xbuf, zbuf, total, meta, wsem,
                 sent, az_r, ax_r, ad_r, md_r, rd_r, rx_r, rz_r):
    rows, features = tokens_ref.shape
    hidden_units = wg.shape[1]
    experts = 4 * nz
    chunk = 4 * rows
    sub = rows // pieces
    halves, half = part.shape[1], part.shape[5]
    f32, bf16 = jnp.float32, jnp.bfloat16
    me = lax.axis_index("ep")
    core = lax.rem(me, 2)
    x = lax.rem(lax.div(me, 2), 2)
    z = lax.div(me, 4)
    d_peer = me + 1 - 2 * core
    x_peer = me + 2 - 4 * x
    has_below, has_above = z > 0, z < nz - 1
    inner = jnp.logical_and(has_below, has_above)
    outer = jnp.logical_not(inner)

    def weight_copy(which, j):
        src, dst = ((wg_hbm, wg), (wu_hbm, wu), (wd_hbm, wd))[which]
        cols = pl.ds(pl.multiple_of(j * tile, tile), tile)
        return pltpu.make_async_copy(src.at[0, :, cols], dst.at[:, cols], wsem.at[which, j])

    barrier = pltpu.get_barrier_semaphore()

    def greet(peer):
        pl.semaphore_signal(barrier, inc=1, device_id={"ep": peer}, device_id_type=MESH)

    greet(d_peer)
    greet(x_peer)
    pl.when(has_below)(lambda: greet(me - 4))
    pl.when(has_above)(lambda: greet(me + 4))

    gu_tiles, d_tiles = hidden_units // tile, features // tile
    for j in range(gu_tiles):
        weight_copy(0, j).start()
        weight_copy(1, j).start()
    for j in range(d_tiles):
        weight_copy(2, j).start()

    own = pl.ds(pl.multiple_of(me * rows, rows), rows)
    tok = tokens_ref[...].astype(f32)
    inverse = lax.rsqrt(jnp.mean(tok * tok, axis=1, keepdims=True) + EPS)
    buf[own, :] = (tok * inverse * gain_ref[...]).astype(bf16)
    lanes = lax.broadcasted_iota(jnp.int32, (experts, rows), 0)
    spread = jnp.zeros((experts, rows), f32)
    for k in range(routes_ref.shape[0]):
        spread = spread + jnp.where(lanes == routes_ref[k:k + 1, :], rw_ref[k:k + 1, :], 0.0)
    meta[me, :, :rows] = spread[:experts // 2]
    meta[me, :, rows:] = spread[experts // 2:]

    pl.semaphore_wait(barrier, jnp.where(inner, 4, 3))

    def remote(src, dst, s, r, dev):
        return pltpu.make_async_remote_copy(
            src_ref=src, dst_ref=dst, send_sem=s, recv_sem=r, device_id={"ep": dev}, device_id_type=MESH
        )

    own_step = nz - 1

    def order(q):
        edge = 0 if 2 * q < nz else nz - 1
        far = nz - 1 - edge
        if q == edge:
            return sorted((p for p in range(nz) if p != q), key=lambda p: abs(p - q))
        return [edge] + [p for p in range(nz) if p not in (q, edge, far)] + [far]

    tables = [order(q) for q in range(nz)]
    places = []
    for i in range(own_step):
        value = tables[0][i]
        for q in range(1, nz):
            value = jnp.where(z == q, tables[q][i], value)
        places.append(value)
    places.append(z)

    def block_of(i, same_x, same_core):
        col = x if same_x else 1 - x
        lane = core if same_core else 1 - core
        return places[i] * 4 + col * 2 + lane

    def rows_of(i, same_x, same_core, q=None):
        at = block_of(i, same_x, same_core) * rows
        if q is None:
            return buf.at[pl.ds(pl.multiple_of(at, rows), rows), :]
        return buf.at[pl.ds(pl.multiple_of(at + q * sub, sub), sub), :]

    def piece(i, same_x, q):
        if q is META:
            return meta.at[block_of(i, same_x, True)]
        return rows_of(i, same_x, True, q)

    def slot_of(q):
        return pieces if q is META else q

    def ag_z(i, q, up):
        ref = piece(i, True, q)
        peer = me + 4 if up else me - 4
        return remote(ref, ref, sent.at[int(up) + (2 if q is META else 0)], az_r.at[places[i], slot_of(q)], peer)

    def ag_x(i, q, arriving=False):
        ref = piece(i, not arriving, q)
        return remote(ref, ref, sent.at[5 if q is META else 4], ax_r.at[i, slot_of(q)], x_peer)

    def ag_d(i, j, q):
        ref = piece(i, j == 0, q)
        r = md_r if q is META else ad_r
        return remote(ref, ref, sent.at[7 if q is META else 6], r.at[i, j], d_peer)

    def ag_d_all(i, j):
        ref = rows_of(i, j == 0, False)
        return remote(ref, ref, sent.at[6], ad_r.at[i, j], d_peer)

    def meta_arrives(i, j):
        ref = meta.at[block_of(i, j == 0, False)]
        remote(ref, ref, sent.at[7], md_r.at[i, j], d_peer).wait_recv()

    def sent_all(ref, n):
        remote(ref, ref, sent.at[n], sent.at[n], d_peer).wait_send()

    def gather_sent():
        for k in range(nz):
            @pl.when(z == k)
            def _():
                for up, blocks in ((0, nz - k if k > 0 else 0), (1, k + 1 if k < nz - 1 else 0)):
                    if blocks:
                        sent_all(buf.at[pl.ds(0, blocks * rows), :], up)
                        sent_all(meta.at[pl.ds(0, blocks)], up + 2)
        sent_all(buf.at[pl.ds(0, nz * rows), :], 4)
        sent_all(meta.at[pl.ds(0, nz)], 5)
        sent_all(buf.at[pl.ds(0, 2 * nz * rows), :], 6)
        sent_all(meta.at[pl.ds(0, 2 * nz)], 7)

    def start(copy):
        copy.start()

    def send_up(i, q, action):
        cond = has_above if i == own_step else jnp.logical_and(has_above, places[i] < z)
        pl.when(cond)(lambda: action(ag_z(i, q, True)))

    def send_down(i, q, action):
        cond = has_below if i == own_step else jnp.logical_and(has_below, places[i] > z)
        pl.when(cond)(lambda: action(ag_z(i, q, False)))

    def pass_on(i, q, action):
        send_up(i, q, action)
        send_down(i, q, action)

    def z_in(i, q):
        ag_z(i, q, True).wait_recv()
        pass_on(i, q, start)
        ag_d(i, 0, q).start()

    def x_out(i, q):
        ag_x(i, q).start()

    def x_in(i, q):
        ag_x(i, q, True).wait_recv()
        ag_d(i, 1, q).start()

    def rs_block(i, j, same_x):
        return part.at[i, j, x if same_x else 1 - x, core]

    def rs_d(i, j):
        return remote(part.at[i, j, :, 1 - core], dbuf.at[i, j], sent.at[8], rd_r.at[i, j], d_peer)

    def rs_x(i, j):
        return remote(rs_block(i, j, False), xbuf.at[i, j], sent.at[9], rx_r.at[i, j], x_peer)

    def rs_z(i, j):
        level, slot = places[i], z
        if i >= 1:
            level = jnp.where(outer, places[0], level)
            slot = jnp.where(outer, nz + i - 1, slot)
        peer = level * 4 + x * 2 + core
        return remote(rs_block(i, j, True), zbuf.at[slot, j], sent.at[10], rz_r.at[slot, j], peer)

    def rs_z_arriving(slot, j):
        ref = zbuf.at[slot, j]
        return remote(ref, ref, sent.at[10], rz_r.at[slot, j], x_peer)

    def chunk_rows(i):
        return pl.ds(pl.multiple_of(places[i] * chunk, chunk), chunk)

    def gate_up_rows(source, kept, target, j, width):
        cols = pl.ds(pl.multiple_of(j * width, width), width)
        lhs = buf[source, :]
        g = jnp.dot(lhs, wg[:, cols], preferred_element_type=f32)
        u = jnp.dot(lhs, wu[:, cols], preferred_element_type=f32)
        kept[target, cols] = (g / (1.0 + jnp.exp(-g)) * u).astype(bf16)

    def gate_up(i, j):
        gate_up_rows(chunk_rows(i), hid, pl.ds(0, chunk), j, 2 * tile)

    def gate_up_chip(j, col, fresh):
        if fresh:
            weight_copy(0, j).wait()
            weight_copy(1, j).wait()
        at = pl.multiple_of(col * (2 * rows), 2 * rows)
        start_row = pl.multiple_of(z * chunk + col * (2 * rows), 2 * rows)
        gate_up_rows(pl.ds(start_row, 2 * rows), hid_own, pl.ds(at, 2 * rows), j, tile)

    def weight_of(i):
        eye = lax.broadcasted_iota(jnp.int32, (rows, rows), 0) == lax.broadcasted_iota(jnp.int32, (rows, rows), 1)
        line, side = lax.rem(me, experts // 2), lax.div(me, experts // 2)
        cols = []
        for b in range(4):
            both = meta[places[i] * 4 + b, pl.ds(line, 1), :]
            row = jnp.where(side == 0, both[:, :rows], both[:, rows:])
            cols.append(jnp.sum(jnp.where(eye, row, 0.0), axis=1, keepdims=True))
        return jnp.concatenate(cols, axis=0)

    def down(i, duties, wide, begin=0, end=halves):
        weight = weight_of(i)
        kept = hid_own if i == own_step else hid

        def body(t, carry):
            cols = pl.ds(pl.multiple_of(t * wide * tile, wide * tile), wide * tile)
            for n in range(wide):
                if i == 0:
                    weight_copy(2, t * wide + n).wait()
            o = jnp.dot(kept[...], wd[:, cols], preferred_element_type=f32)
            for n in range(wide):
                value = (o[:, n * tile:(n + 1) * tile] * weight).astype(bf16)
                part[i, t * wide + n] = value.reshape(2, 2, rows, half)
            for n in range(wide):
                rs_d(i, t * wide + n).start()
            duties(t)
            return carry

        lax.fori_loop(begin // wide, end // wide, body, 0)

    def finish_d(i, j):
        rs_d(i, j).wait_recv()
        ref = rs_block(i, j, False)
        ref[...] = (ref[...].astype(f32) + dbuf[i, j, 1 - x].astype(f32)).astype(bf16)
        rs_x(i, j).start()

    def finish_x(i, j):
        rs_x(i, j).wait_recv()
        ref = rs_block(i, j, True)
        value = ref[...].astype(f32) + dbuf[i, j, x].astype(f32) + xbuf[i, j].astype(f32)
        if i == own_step:
            total[j] = value
        else:
            ref[...] = value.astype(bf16)
            if i >= 1:
                @pl.when(inner)
                def _():
                    rs_z_arriving(nz + i - 1, j).wait_recv()
                    ref[...] = (value + zbuf[nz + i - 1, j].astype(f32)).astype(bf16)
            rs_z(i, j).start()

    def loop(i, duties):
        def body(j, carry):
            gate_up(i, j)
            duties(j)
            return carry

        lax.fori_loop(0, gu_tiles // 2, body, 0)

    def chunk_ready(i):
        for j in range(2):
            ag_d_all(i, j).wait_recv()

    def step(body):
        lax.fori_loop(0, pieces, lambda j, carry: (body(j), carry)[1], 0)

    for q in [META] + list(range(pieces)):
        x_out(own_step, q)
        pass_on(own_step, q, start)
        ag_d(own_step, 0, q).start()

    z_in(0, META)
    x_out(0, META)

    @pl.when(inner)
    def _():
        z_in(1, META)
        x_out(1, META)

    ag_d_all(own_step, 0).wait_recv()

    def gather(q):
        gate_up_chip(q, x, True)
        x_in(own_step, q)
        z_in(0, q)
        x_out(0, q)
        pl.when(inner)(lambda: z_in(1, q))

    step(gather)

    @pl.when(inner)
    def _():
        z_in(2, META)
        x_out(2, META)

    @pl.when(outer)
    def _():
        z_in(1, META)
        x_out(1, META)

    ag_d_all(own_step, 1).wait_recv()

    def own_rest(j):
        gate_up_chip(j, 1 - x, False)
        pl.when(inner)(lambda: z_in(2, j))
        pl.when(outer)(lambda: z_in(1, j))
        x_out(1, j)
        x_in(0, j)

    step(own_rest)

    @pl.when(inner)
    def _():
        for q in range(pieces):
            x_out(2, q)

    @pl.when(outer)
    def _():
        z_in(2, META)
        x_out(2, META)

    x_in(own_step, META)
    x_in(0, META)
    chunk_ready(0)

    def both(action, j):
        action(2 * j)
        action(2 * j + 1)

    def far_in(q):
        z_in(2, q)
        x_out(2, q)

    def duties_0(j):
        pl.when(outer)(lambda: both(far_in, j))

        @pl.when(j == 0)
        def _():
            x_in(1, 0)

        @pl.when(j == 1)
        def _():
            x_in(1, 1)
            x_in(1, 2)

    loop(0, duties_0)
    for j in range(2):
        meta_arrives(0, j)

    def down_duties_0(t):
        pl.when(t == 0)(lambda: x_in(1, 3))
        pl.when(t == 1)(lambda: both(lambda j: finish_d(0, j), 0))

    down(0, down_duties_0, 2)
    x_in(1, META)
    chunk_ready(1)

    def duties_1(j):
        pl.when(j == 0)(lambda: both(lambda q: finish_d(0, q), 1))
        both(lambda q: x_in(2, q), j)

    loop(1, duties_1)
    x_in(2, META)
    for j in range(2):
        meta_arrives(1, j)

    def down_duties_1(t):
        pl.when(t == 1)(lambda: both(lambda j: finish_d(1, j), 0))
        both(lambda j: finish_x(0, j), t)

    down(1, down_duties_1, 2)
    chunk_ready(2)

    def duties_2(j):
        pl.when(j == 0)(lambda: both(lambda q: finish_d(1, q), 1))
        pl.when(jnp.logical_and(j == 1, outer))(lambda: finish_x(1, 0))

    loop(2, duties_2)
    for i in (2, own_step):
        for j in range(2):
            meta_arrives(i, j)

    def down_duties_2(t):
        pl.when(t >= 2)(lambda: finish_d(2, t - 2))
        pl.when(jnp.logical_and(t < 3, outer))(lambda: finish_x(1, t + 1))

    down(2, down_duties_2, 1)

    def down_duties_own(t):
        pl.when(t < 2)(lambda: finish_d(2, t + 2))
        pl.when(t >= 2)(lambda: finish_d(own_step, t - 2))
        pl.when(inner)(lambda: finish_x(1, t))

    down(own_step, down_duties_own, 1)
    finish_x(2, 0)
    finish_d(own_step, 2)
    finish_x(2, 1)
    finish_d(own_step, 3)
    finish_x(2, 2)
    finish_x(2, 3)
    gather_sent()
    step(lambda j: finish_x(own_step, j))

    def collect(level, cond):
        def one(j):
            rs_z_arriving(level, j).wait_recv()
            total[j] = total[j] + zbuf[level, j].astype(f32)

        pl.when(cond)(lambda: step(one))

    for level in range(nz):
        if level in (0, nz - 1):
            collect(level, z == (1 if level == 0 else nz - 2))
        else:
            collect(level, z != level)

    squares = 0.0
    for j in range(halves):
        squares = squares + jnp.sum(total[j] * total[j], axis=1, keepdims=True)
    inverse_out = lax.rsqrt(squares / features + EPS)
    for j in range(halves):
        cols = pl.ds(j * half, half)
        out_ref[:, cols] = (total[j] * inverse_out * fgain_ref[:, cols]).astype(out_ref.dtype)

    sent_all(dbuf, 8)
    sent_all(xbuf, 9)
    sent_all(zbuf.at[pl.ds(0, own_step)], 10)


def fused_device(tokens, norm_gain, routes, route_weights, w_gate, w_up, w_down, final_gain):
    rows, features = tokens.shape
    hidden_units = w_gate.shape[2]
    experts = lax.axis_size("ep")
    nz = experts // 4
    pieces, halves = 4, 4
    tile = hidden_units // pieces
    half = features // halves
    vmem, anywhere = pl.BlockSpec(memory_space=pltpu.VMEM), pl.BlockSpec(memory_space=pl.ANY)
    dma = pltpu.SemaphoreType.DMA
    bf16 = jnp.bfloat16
    return pl.pallas_call(
        functools.partial(fused_kernel, nz, tile, pieces),
        out_shape=jax.ShapeDtypeStruct((rows, features), jnp.bfloat16),
        in_specs=[vmem, vmem, vmem, vmem, anywhere, anywhere, anywhere, vmem],
        out_specs=vmem,
        scratch_shapes=[
            pltpu.VMEM((experts * rows, features), bf16),
            pltpu.VMEM((features, hidden_units), bf16),
            pltpu.VMEM((features, hidden_units), bf16),
            pltpu.VMEM((hidden_units, features), bf16),
            pltpu.VMEM((4 * rows, hidden_units), bf16),
            pltpu.VMEM((4 * rows, hidden_units), bf16),
            pltpu.VMEM((nz, halves, 2, 2, rows, half), bf16),
            pltpu.VMEM((nz, halves, 2, rows, half), bf16),
            pltpu.VMEM((nz, halves, rows, half), bf16),
            pltpu.VMEM((nz + 2, halves, rows, half), bf16),
            pltpu.VMEM((halves, rows, half), jnp.float32),
            pltpu.VMEM((experts, experts // 2, 2 * rows), jnp.float32),
            dma((3, max(hidden_units, features) // tile)),
            dma((11,)), dma((nz, pieces + 1)), dma((nz, pieces + 1)), dma((nz, 2)), dma((nz, 2)),
            dma((nz, halves)), dma((nz, halves)), dma((nz + 2, halves)),
        ],
        compiler_params=pltpu.CompilerParams(
            collective_id=0, has_side_effects=True, vmem_limit_bytes=60 * 1024 * 1024
        ),
    )(tokens, norm_gain[None, :], routes.T, route_weights.T, w_gate, w_up, w_down, final_gain[None, :])


def solution(mesh):
    placed = (
        P(("grp", "ep"), None),
        P(),
        P(("grp", "ep"), None),
        P(("grp", "ep"), None),
        P("ep", None, "tp"),
        P("ep", None, "tp"),
        P("ep", "tp", None),
        P("tp"),
    )
    ep, tp = mesh.shape["ep"], mesh.shape["tp"]

    def step(*args):
        rows, features = args[0].shape
        hidden_units = args[4].shape[2]
        fits = 3 * features * hidden_units + 3 * ep * rows * features < 24 * 2 ** 20
        whole_tiles = features % 2048 == 0 and hidden_units % 2048 == 0 and rows % 64 == 0
        if tp == 1 and ep == 16 and args[4].shape[0] == 1 and fits and whole_tiles:
            return fused_device(*args)
        return per_device(*args)

    return jax.shard_map(
        step, mesh=mesh, in_specs=placed, out_specs=P(("grp", "ep"), "tp"), check_vma=False
    )
```

```python
import functools

import jax
import jax.numpy as jnp
from jax import lax
from jax.experimental import pallas as pl
from jax.experimental.pallas import tpu as pltpu
from jax.sharding import PartitionSpec as P

TOP_K = 6


EPS = 1e-06
MESH = pl.DeviceIdType.MESH
META = None


def slot_table(route_rows, experts_all, capacity):
    flattened = route_rows.reshape(-1)
    matches = (flattened[:, None] == jnp.arange(experts_all, dtype=jnp.int32)[None, :]).astype(
        jnp.int32
    )
    earlier = jnp.cumsum(matches, axis=0) - matches
    slot_of = jnp.sum(earlier * matches, axis=1)
    return (flattened * capacity + slot_of).reshape(route_rows.shape)


def per_device(tokens, norm_gain, routes, route_weights, w_gate, w_up, w_down, final_gain):
    tok_count, features = tokens.shape
    ep_size = lax.axis_size("ep")
    exp_local = w_gate.shape[0]
    experts_all = exp_local * ep_size
    capacity = max(2, min(tok_count, 2 * tok_count * TOP_K // experts_all))
    slot_count = experts_all * capacity
    tokens_f = tokens.astype(jnp.float32)
    inverse = lax.rsqrt(jnp.mean(tokens_f * tokens_f, axis=1, keepdims=True) + EPS)
    normed = (tokens_f * inverse * norm_gain[None, :]).astype(jnp.bfloat16)
    places = slot_table(routes, experts_all, capacity)
    slot_ids = jnp.arange(slot_count, dtype=jnp.int32)
    matched = places[:, :, None] == slot_ids[None, None, :]
    selector = jnp.sum(matched.astype(jnp.float32), axis=1).T.astype(jnp.bfloat16)
    combine_rows = jnp.sum(jnp.where(matched, route_weights[:, :, None], 0.0), axis=1)
    outgoing = jnp.dot(selector, normed, preferred_element_type=jnp.float32).astype(jnp.bfloat16)
    outgoing = outgoing.reshape(ep_size, exp_local, capacity, features)
    received = lax.all_to_all(outgoing, "ep", split_axis=0, concat_axis=0, tiled=True)
    gate_value = jnp.einsum("secd,edf->secf", received, w_gate, preferred_element_type=jnp.float32)
    up_value = jnp.einsum("secd,edf->secf", received, w_up, preferred_element_type=jnp.float32)
    hidden = (jax.nn.silu(gate_value) * up_value).astype(jnp.bfloat16)
    partial_value = jnp.einsum("secf,efd->secd", hidden, w_down, preferred_element_type=jnp.float32)
    summed = lax.psum_scatter(
        partial_value.astype(jnp.bfloat16), "tp", scatter_dimension=3, tiled=True
    )
    returned = lax.all_to_all(summed, "ep", split_axis=0, concat_axis=0, tiled=True)
    results = returned.reshape(slot_count, returned.shape[3]).astype(jnp.float32)
    combined = jnp.dot(combine_rows, results, precision=lax.Precision.HIGHEST)
    local_squares = jnp.sum(combined * combined, axis=1)
    squares_all = lax.psum(local_squares, "tp")
    inverse_out = lax.rsqrt(squares_all / features + EPS)
    return (combined * inverse_out[:, None] * final_gain[None, :]).astype(jnp.bfloat16)


def fused_kernel(nz, tile, pieces, tokens_hbm, gain_hbm, routes_hbm, rw_hbm, wg_hbm, wu_hbm, wd_hbm, fgain_hbm,
                 out_ref, tokens_ref, gain_ref, routes_ref, rw_ref, fgain_ref, small, buf, wg, wu, wd, hid, hid_own, part, dbuf, xbuf, zbuf, total, meta, wsem,
                 sent, az_r, ax_r, ad_r, md_r, rd_r, rx_r, rz_r):
    rows, features = tokens_ref.shape
    hidden_units = wg.shape[1]
    experts = 4 * nz
    chunk = 4 * rows
    sub = rows // pieces
    halves, half = part.shape[1], part.shape[5]
    f32, bf16 = jnp.float32, jnp.bfloat16
    me = lax.axis_index("ep")
    core = lax.rem(me, 2)
    x = lax.rem(lax.div(me, 2), 2)
    z = lax.div(me, 4)
    d_peer = me + 1 - 2 * core
    x_peer = me + 2 - 4 * x
    has_below, has_above = z > 0, z < nz - 1
    inner = jnp.logical_and(has_below, has_above)
    outer = jnp.logical_not(inner)

    def weight_copy(which, j):
        src, dst = ((wg_hbm, wg), (wu_hbm, wu), (wd_hbm, wd))[which]
        cols = pl.ds(pl.multiple_of(j * tile, tile), tile)
        return pltpu.make_async_copy(src.at[0, :, cols], dst.at[:, cols], wsem.at[which, j])

    barrier = pltpu.get_barrier_semaphore()

    def greet(peer):
        pl.semaphore_signal(barrier, inc=1, device_id={"ep": peer}, device_id_type=MESH)

    greet(d_peer)
    greet(x_peer)
    pl.when(has_below)(lambda: greet(me - 4))
    pl.when(has_above)(lambda: greet(me + 4))

    loads = [
        pltpu.make_async_copy(src, dst, small.at[n])
        for n, (src, dst) in enumerate((
            (tokens_hbm, tokens_ref), (gain_hbm, gain_ref), (routes_hbm, routes_ref), (rw_hbm, rw_ref),
            (fgain_hbm, fgain_ref),
        ))
    ]
    for load in loads:
        load.start()

    gu_tiles, d_tiles = hidden_units // tile, features // tile
    for j in range(gu_tiles):
        weight_copy(0, j).start(priority=1)
        weight_copy(1, j).start(priority=1)
    for j in range(d_tiles):
        weight_copy(2, j).start(priority=1)

    for load in loads:
        load.wait()
    own = pl.ds(pl.multiple_of(me * rows, rows), rows)
    tok = tokens_ref[...].astype(f32)
    inverse = lax.rsqrt(jnp.mean(tok * tok, axis=1, keepdims=True) + EPS)
    buf[own, :] = (tok * inverse * gain_ref[...]).astype(bf16)
    lanes = lax.broadcasted_iota(jnp.int32, (experts, rows), 0)
    spread = jnp.zeros((experts, rows), f32)
    for k in range(routes_ref.shape[0]):
        spread = spread + jnp.where(lanes == routes_ref[k:k + 1, :], rw_ref[k:k + 1, :], 0.0)
    meta[me, :, :rows] = spread[:experts // 2]
    meta[me, :, rows:] = spread[experts // 2:]

    pl.semaphore_wait(barrier, jnp.where(inner, 4, 3))

    def remote(src, dst, s, r, dev):
        return pltpu.make_async_remote_copy(
            src_ref=src, dst_ref=dst, send_sem=s, recv_sem=r, device_id={"ep": dev}, device_id_type=MESH
        )

    own_step = nz - 1

    def order(q):
        edge = 0 if 2 * q < nz else nz - 1
        far = nz - 1 - edge
        if q == edge:
            return sorted((p for p in range(nz) if p != q), key=lambda p: abs(p - q))
        return [edge] + [p for p in range(nz) if p not in (q, edge, far)] + [far]

    tables = [order(q) for q in range(nz)]
    places = []
    for i in range(own_step):
        value = tables[0][i]
        for q in range(1, nz):
            value = jnp.where(z == q, tables[q][i], value)
        places.append(value)
    places.append(z)

    def block_of(i, same_x, same_core):
        col = x if same_x else 1 - x
        lane = core if same_core else 1 - core
        return places[i] * 4 + col * 2 + lane

    def rows_of(i, same_x, same_core, q=None):
        at = block_of(i, same_x, same_core) * rows
        if q is None:
            return buf.at[pl.ds(pl.multiple_of(at, rows), rows), :]
        return buf.at[pl.ds(pl.multiple_of(at + q * sub, sub), sub), :]

    def piece(i, same_x, q):
        if q is META:
            return meta.at[block_of(i, same_x, True)]
        return rows_of(i, same_x, True, q)

    def slot_of(q):
        return pieces if q is META else q

    def ag_z(i, q, up):
        ref = piece(i, True, q)
        peer = me + 4 if up else me - 4
        return remote(ref, ref, sent.at[int(up) + (2 if q is META else 0)], az_r.at[places[i], slot_of(q)], peer)

    def ag_x(i, q, arriving=False):
        ref = piece(i, not arriving, q)
        return remote(ref, ref, sent.at[5 if q is META else 4], ax_r.at[i, slot_of(q)], x_peer)

    def ag_d(i, j, q):
        ref = piece(i, j == 0, q)
        r = md_r if q is META else ad_r
        return remote(ref, ref, sent.at[7 if q is META else 6], r.at[i, j], d_peer)

    def ag_d_all(i, j):
        ref = rows_of(i, j == 0, False)
        return remote(ref, ref, sent.at[6], ad_r.at[i, j], d_peer)

    def meta_arrives(i, j):
        ref = meta.at[block_of(i, j == 0, False)]
        remote(ref, ref, sent.at[7], md_r.at[i, j], d_peer).wait_recv()

    def sent_all(ref, n):
        remote(ref, ref, sent.at[n], sent.at[n], d_peer).wait_send()

    def gather_sent():
        for k in range(nz):
            @pl.when(z == k)
            def _():
                for up, blocks in ((0, nz - k if k > 0 else 0), (1, k + 1 if k < nz - 1 else 0)):
                    if blocks:
                        sent_all(buf.at[pl.ds(0, blocks * rows), :], up)
                        sent_all(meta.at[pl.ds(0, blocks)], up + 2)
        sent_all(buf.at[pl.ds(0, nz * rows), :], 4)
        sent_all(meta.at[pl.ds(0, nz)], 5)
        sent_all(buf.at[pl.ds(0, 2 * nz * rows), :], 6)
        sent_all(meta.at[pl.ds(0, 2 * nz)], 7)

    def start(copy):
        copy.start()

    def send_up(i, q, action):
        cond = has_above if i == own_step else jnp.logical_and(has_above, places[i] < z)
        pl.when(cond)(lambda: action(ag_z(i, q, True)))

    def send_down(i, q, action):
        cond = has_below if i == own_step else jnp.logical_and(has_below, places[i] > z)
        pl.when(cond)(lambda: action(ag_z(i, q, False)))

    def pass_on(i, q, action):
        send_up(i, q, action)
        send_down(i, q, action)

    def z_in(i, q):
        ag_z(i, q, True).wait_recv()
        pass_on(i, q, start)
        ag_d(i, 0, q).start()

    def x_out(i, q):
        ag_x(i, q).start()

    def x_in(i, q):
        ag_x(i, q, True).wait_recv()
        ag_d(i, 1, q).start()

    def rs_block(i, j, same_x):
        return part.at[i, j, x if same_x else 1 - x, core]

    def rs_d(i, j):
        return remote(part.at[i, j, :, 1 - core], dbuf.at[i, j], sent.at[8], rd_r.at[i, j], d_peer)

    def rs_x(i, j):
        return remote(rs_block(i, j, False), xbuf.at[i, j], sent.at[9], rx_r.at[i, j], x_peer)

    def rs_z(i, j):
        level, slot = places[i], z
        if i >= 1:
            level = jnp.where(outer, places[0], level)
            slot = jnp.where(outer, nz + i - 1, slot)
        peer = level * 4 + x * 2 + core
        return remote(rs_block(i, j, True), zbuf.at[slot, j], sent.at[10], rz_r.at[slot, j], peer)

    def rs_z_arriving(slot, j):
        ref = zbuf.at[slot, j]
        return remote(ref, ref, sent.at[10], rz_r.at[slot, j], x_peer)

    def chunk_rows(i):
        return pl.ds(pl.multiple_of(places[i] * chunk, chunk), chunk)

    def gate_up_rows(source, kept, target, j, width):
        cols = pl.ds(pl.multiple_of(j * width, width), width)
        lhs = buf[source, :]
        g = jnp.dot(lhs, wg[:, cols], preferred_element_type=f32)
        u = jnp.dot(lhs, wu[:, cols], preferred_element_type=f32)
        kept[target, cols] = (g / (1.0 + jnp.exp(-g)) * u).astype(bf16)

    def gate_up(i, j):
        gate_up_rows(chunk_rows(i), hid, pl.ds(0, chunk), j, 2 * tile)

    def gate_up_chip(j, col, fresh):
        if fresh:
            weight_copy(0, j).wait()
            weight_copy(1, j).wait()
        at = pl.multiple_of(col * (2 * rows), 2 * rows)
        start_row = pl.multiple_of(z * chunk + col * (2 * rows), 2 * rows)
        gate_up_rows(pl.ds(start_row, 2 * rows), hid_own, pl.ds(at, 2 * rows), j, tile)

    def weight_of(i):
        eye = lax.broadcasted_iota(jnp.int32, (rows, rows), 0) == lax.broadcasted_iota(jnp.int32, (rows, rows), 1)
        line, side = lax.rem(me, experts // 2), lax.div(me, experts // 2)
        cols = []
        for b in range(4):
            both = meta[places[i] * 4 + b, pl.ds(line, 1), :]
            row = jnp.where(side == 0, both[:, :rows], both[:, rows:])
            cols.append(jnp.sum(jnp.where(eye, row, 0.0), axis=1, keepdims=True))
        return jnp.concatenate(cols, axis=0)

    def down(i, duties, wide, begin=0, end=halves):
        weight = weight_of(i)
        kept = hid_own if i == own_step else hid

        def body(t, carry):
            cols = pl.ds(pl.multiple_of(t * wide * tile, wide * tile), wide * tile)
            for n in range(wide):
                if i == 0:
                    weight_copy(2, t * wide + n).wait()
            o = jnp.dot(kept[...], wd[:, cols], preferred_element_type=f32)
            for n in range(wide):
                value = (o[:, n * tile:(n + 1) * tile] * weight).astype(bf16)
                part[i, t * wide + n] = value.reshape(2, 2, rows, half)
            for n in range(wide):
                rs_d(i, t * wide + n).start()
            duties(t)
            return carry

        lax.fori_loop(begin // wide, end // wide, body, 0)

    def finish_d(i, j):
        rs_d(i, j).wait_recv()
        ref = rs_block(i, j, False)
        ref[...] = (ref[...].astype(f32) + dbuf[i, j, 1 - x].astype(f32)).astype(bf16)
        rs_x(i, j).start()

    def finish_x(i, j):
        rs_x(i, j).wait_recv()
        ref = rs_block(i, j, True)
        value = ref[...].astype(f32) + dbuf[i, j, x].astype(f32) + xbuf[i, j].astype(f32)
        if i == own_step:
            total[j] = value
        else:
            ref[...] = value.astype(bf16)
            if i >= 1:
                @pl.when(inner)
                def _():
                    rs_z_arriving(nz + i - 1, j).wait_recv()
                    ref[...] = (value + zbuf[nz + i - 1, j].astype(f32)).astype(bf16)
            rs_z(i, j).start()

    def loop(i, duties):
        def body(j, carry):
            gate_up(i, j)
            duties(j)
            return carry

        lax.fori_loop(0, gu_tiles // 2, body, 0)

    def chunk_ready(i):
        for j in range(2):
            ag_d_all(i, j).wait_recv()

    def step(body):
        lax.fori_loop(0, pieces, lambda j, carry: (body(j), carry)[1], 0)

    for q in [META] + list(range(pieces)):
        x_out(own_step, q)
        pass_on(own_step, q, start)
        ag_d(own_step, 0, q).start()

    z_in(0, META)
    x_out(0, META)

    @pl.when(inner)
    def _():
        z_in(1, META)
        x_out(1, META)

    ag_d_all(own_step, 0).wait_recv()

    def gather(q):
        gate_up_chip(q, x, True)
        x_in(own_step, q)
        z_in(0, q)
        x_out(0, q)
        pl.when(inner)(lambda: z_in(1, q))

    step(gather)

    @pl.when(inner)
    def _():
        z_in(2, META)
        x_out(2, META)

    @pl.when(outer)
    def _():
        z_in(1, META)
        x_out(1, META)

    ag_d_all(own_step, 1).wait_recv()

    def own_rest(j):
        gate_up_chip(j, 1 - x, False)
        pl.when(inner)(lambda: z_in(2, j))
        pl.when(outer)(lambda: z_in(1, j))
        x_out(1, j)
        x_in(0, j)

    step(own_rest)

    @pl.when(inner)
    def _():
        for q in range(pieces):
            x_out(2, q)

    @pl.when(outer)
    def _():
        z_in(2, META)
        x_out(2, META)

    x_in(own_step, META)
    x_in(0, META)
    chunk_ready(0)

    def both(action, j):
        action(2 * j)
        action(2 * j + 1)

    def far_in(q):
        z_in(2, q)
        x_out(2, q)

    def duties_0(j):
        pl.when(outer)(lambda: both(far_in, j))

        @pl.when(j == 0)
        def _():
            x_in(1, 0)

        @pl.when(j == 1)
        def _():
            x_in(1, 1)
            x_in(1, 2)

    loop(0, duties_0)
    for j in range(2):
        meta_arrives(0, j)

    def down_duties_0(t):
        pl.when(t == 0)(lambda: x_in(1, 3))

    down(0, down_duties_0, 2)
    x_in(1, META)
    chunk_ready(1)

    def duties_1(j):
        both(lambda q: finish_d(0, q), j)
        both(lambda q: x_in(2, q), j)

    loop(1, duties_1)
    x_in(2, META)
    for j in range(2):
        meta_arrives(1, j)

    def down_duties_1(t):
        pl.when(t == 1)(lambda: both(lambda j: finish_d(1, j), 0))
        pl.when(t == 1)(lambda: both(lambda j: finish_x(0, j), 0))

    down(1, down_duties_1, 2)
    chunk_ready(2)

    def duties_2(j):
        @pl.when(j == 0)
        def _():
            both(lambda q: finish_d(1, q), 1)
            both(lambda q: finish_x(0, q), 1)

        pl.when(jnp.logical_and(j == 1, outer))(lambda: finish_x(1, 0))

    loop(2, duties_2)
    for i in (2, own_step):
        for j in range(2):
            meta_arrives(i, j)

    def down_duties_2(t):
        pl.when(t >= 2)(lambda: finish_d(2, t - 2))
        pl.when(jnp.logical_and(t < 3, outer))(lambda: finish_x(1, t + 1))

    down(2, down_duties_2, 1)

    def down_duties_own(t):
        pl.when(t < 2)(lambda: finish_d(2, t + 2))
        pl.when(t >= 2)(lambda: finish_d(own_step, t - 2))
        pl.when(inner)(lambda: finish_x(1, t))

    down(own_step, down_duties_own, 1)
    finish_x(2, 0)
    finish_d(own_step, 2)
    finish_x(2, 1)
    finish_d(own_step, 3)
    finish_x(2, 2)
    finish_x(2, 3)
    gather_sent()
    step(lambda j: finish_x(own_step, j))

    def collect(level, cond):
        def one(j):
            rs_z_arriving(level, j).wait_recv()
            total[j] = total[j] + zbuf[level, j].astype(f32)

        pl.when(cond)(lambda: step(one))

    for level in range(nz):
        if level in (0, nz - 1):
            collect(level, z == (1 if level == 0 else nz - 2))
        else:
            collect(level, z != level)

    squares = 0.0
    for j in range(halves):
        squares = squares + jnp.sum(total[j] * total[j], axis=1, keepdims=True)
    inverse_out = lax.rsqrt(squares / features + EPS)
    for j in range(halves):
        cols = pl.ds(j * half, half)
        out_ref[:, cols] = (total[j] * inverse_out * fgain_ref[:, cols]).astype(out_ref.dtype)

    sent_all(dbuf, 8)
    sent_all(xbuf, 9)
    sent_all(zbuf.at[pl.ds(0, own_step)], 10)


def fused_device(tokens, norm_gain, routes, route_weights, w_gate, w_up, w_down, final_gain):
    rows, features = tokens.shape
    hidden_units = w_gate.shape[2]
    experts = lax.axis_size("ep")
    nz = experts // 4
    pieces, halves = 4, 4
    tile = hidden_units // pieces
    half = features // halves
    vmem, hbm = pl.BlockSpec(memory_space=pltpu.VMEM), pl.BlockSpec(memory_space=pltpu.HBM)
    dma = pltpu.SemaphoreType.DMA
    bf16 = jnp.bfloat16
    return pl.pallas_call(
        functools.partial(fused_kernel, nz, tile, pieces),
        out_shape=jax.ShapeDtypeStruct((rows, features), jnp.bfloat16),
        in_specs=[hbm] * 8,
        out_specs=vmem,
        scratch_shapes=[
            pltpu.VMEM((rows, features), bf16),
            pltpu.VMEM((1, features), jnp.float32),
            pltpu.VMEM(routes.shape[::-1], jnp.int32),
            pltpu.VMEM(routes.shape[::-1], jnp.float32),
            pltpu.VMEM((1, features), jnp.float32),
            dma((5,)),
            pltpu.VMEM((experts * rows, features), bf16),
            pltpu.VMEM((features, hidden_units), bf16),
            pltpu.VMEM((features, hidden_units), bf16),
            pltpu.VMEM((hidden_units, features), bf16),
            pltpu.VMEM((4 * rows, hidden_units), bf16),
            pltpu.VMEM((4 * rows, hidden_units), bf16),
            pltpu.VMEM((nz, halves, 2, 2, rows, half), bf16),
            pltpu.VMEM((nz, halves, 2, rows, half), bf16),
            pltpu.VMEM((nz, halves, rows, half), bf16),
            pltpu.VMEM((nz + 2, halves, rows, half), bf16),
            pltpu.VMEM((halves, rows, half), jnp.float32),
            pltpu.VMEM((experts, experts // 2, 2 * rows), jnp.float32),
            dma((3, max(hidden_units, features) // tile)),
            dma((11,)), dma((nz, pieces + 1)), dma((nz, pieces + 1)), dma((nz, 2)), dma((nz, 2)),
            dma((nz, halves)), dma((nz, halves)), dma((nz + 2, halves)),
        ],
        compiler_params=pltpu.CompilerParams(
            collective_id=0, has_side_effects=True, vmem_limit_bytes=48 * 1024 * 1024
        ),
    )(*(
        pltpu.with_memory_space_constraint(array, pltpu.HBM)
        for array in (
            tokens, norm_gain[None, :], routes.T, route_weights.T, w_gate, w_up, w_down, final_gain[None, :],
        )
    ))


def solution(mesh):
    placed = (
        P(("grp", "ep"), None),
        P(),
        P(("grp", "ep"), None),
        P(("grp", "ep"), None),
        P("ep", None, "tp"),
        P("ep", None, "tp"),
        P("ep", "tp", None),
        P("tp"),
    )
    ep, tp = mesh.shape["ep"], mesh.shape["tp"]

    def step(*args):
        rows, features = args[0].shape
        hidden_units = args[4].shape[2]
        fits = 3 * features * hidden_units + 3 * ep * rows * features < 24 * 2 ** 20
        whole_tiles = features % 2048 == 0 and hidden_units % 2048 == 0 and rows % 64 == 0
        if tp == 1 and ep == 16 and args[4].shape[0] == 1 and fits and whole_tiles:
            return fused_device(*args)
        return per_device(*args)

    return jax.shard_map(
        step, mesh=mesh, in_specs=placed, out_specs=P(("grp", "ep"), "tp"), check_vma=False
    )
```

```python
import functools

import jax
import jax.numpy as jnp
from jax import lax
from jax.experimental import pallas as pl
from jax.experimental.pallas import tpu as pltpu
from jax.sharding import PartitionSpec as P

TOP_K = 6


EPS = 1e-06
MESH = pl.DeviceIdType.MESH
META = None


def slot_table(route_rows, experts_all, capacity):
    flattened = route_rows.reshape(-1)
    matches = (flattened[:, None] == jnp.arange(experts_all, dtype=jnp.int32)[None, :]).astype(
        jnp.int32
    )
    earlier = jnp.cumsum(matches, axis=0) - matches
    slot_of = jnp.sum(earlier * matches, axis=1)
    return (flattened * capacity + slot_of).reshape(route_rows.shape)


def per_device(tokens, norm_gain, routes, route_weights, w_gate, w_up, w_down, final_gain):
    tok_count, features = tokens.shape
    ep_size = lax.axis_size("ep")
    exp_local = w_gate.shape[0]
    experts_all = exp_local * ep_size
    capacity = max(2, min(tok_count, 2 * tok_count * TOP_K // experts_all))
    slot_count = experts_all * capacity
    tokens_f = tokens.astype(jnp.float32)
    inverse = lax.rsqrt(jnp.mean(tokens_f * tokens_f, axis=1, keepdims=True) + EPS)
    normed = (tokens_f * inverse * norm_gain[None, :]).astype(jnp.bfloat16)
    places = slot_table(routes, experts_all, capacity)
    slot_ids = jnp.arange(slot_count, dtype=jnp.int32)
    matched = places[:, :, None] == slot_ids[None, None, :]
    selector = jnp.sum(matched.astype(jnp.float32), axis=1).T.astype(jnp.bfloat16)
    combine_rows = jnp.sum(jnp.where(matched, route_weights[:, :, None], 0.0), axis=1)
    outgoing = jnp.dot(selector, normed, preferred_element_type=jnp.float32).astype(jnp.bfloat16)
    outgoing = outgoing.reshape(ep_size, exp_local, capacity, features)
    received = lax.all_to_all(outgoing, "ep", split_axis=0, concat_axis=0, tiled=True)
    gate_value = jnp.einsum("secd,edf->secf", received, w_gate, preferred_element_type=jnp.float32)
    up_value = jnp.einsum("secd,edf->secf", received, w_up, preferred_element_type=jnp.float32)
    hidden = (jax.nn.silu(gate_value) * up_value).astype(jnp.bfloat16)
    partial_value = jnp.einsum("secf,efd->secd", hidden, w_down, preferred_element_type=jnp.float32)
    summed = lax.psum_scatter(
        partial_value.astype(jnp.bfloat16), "tp", scatter_dimension=3, tiled=True
    )
    returned = lax.all_to_all(summed, "ep", split_axis=0, concat_axis=0, tiled=True)
    results = returned.reshape(slot_count, returned.shape[3]).astype(jnp.float32)
    combined = jnp.dot(combine_rows, results, precision=lax.Precision.HIGHEST)
    local_squares = jnp.sum(combined * combined, axis=1)
    squares_all = lax.psum(local_squares, "tp")
    inverse_out = lax.rsqrt(squares_all / features + EPS)
    return (combined * inverse_out[:, None] * final_gain[None, :]).astype(jnp.bfloat16)


def fused_kernel(nz, tile, pieces, tokens_hbm, gain_hbm, routes_hbm, rw_hbm, wg_hbm, wu_hbm, wd_hbm, fgain_hbm,
                 out_ref, tokens_ref, gain_ref, routes_ref, rw_ref, fgain_ref, small, buf, wg, wu, wd, hid, hid_own, part, dbuf, xbuf, zbuf, total, meta, wsem,
                 sent, az_r, ax_r, ad_r, md_r, rd_r, rx_r, rz_r):
    rows, features = tokens_ref.shape
    hidden_units = wg.shape[1]
    experts = 4 * nz
    chunk = 4 * rows
    sub = rows // pieces
    halves, half = part.shape[1], part.shape[5]
    f32, bf16 = jnp.float32, jnp.bfloat16
    me = lax.axis_index("ep")
    core = lax.rem(me, 2)
    x = lax.rem(lax.div(me, 2), 2)
    z = lax.div(me, 4)
    d_peer = me + 1 - 2 * core
    x_peer = me + 2 - 4 * x
    has_below, has_above = z > 0, z < nz - 1
    inner = jnp.logical_and(has_below, has_above)
    outer = jnp.logical_not(inner)

    def weight_copy(which, j):
        src, dst = ((wg_hbm, wg), (wu_hbm, wu), (wd_hbm, wd))[which]
        cols = pl.ds(pl.multiple_of(j * tile, tile), tile)
        return pltpu.make_async_copy(src.at[0, :, cols], dst.at[:, cols], wsem.at[which, j])

    barrier = pltpu.get_barrier_semaphore()

    def greet(peer):
        pl.semaphore_signal(barrier, inc=1, device_id={"ep": peer}, device_id_type=MESH)

    greet(d_peer)
    greet(x_peer)
    pl.when(has_below)(lambda: greet(me - 4))
    pl.when(has_above)(lambda: greet(me + 4))

    loads = [
        pltpu.make_async_copy(src, dst, small.at[n])
        for n, (src, dst) in enumerate((
            (tokens_hbm, tokens_ref), (gain_hbm, gain_ref), (routes_hbm, routes_ref), (rw_hbm, rw_ref),
            (fgain_hbm, fgain_ref),
        ))
    ]
    for load in loads:
        load.start()

    gu_tiles, d_tiles = hidden_units // tile, features // tile
    for j in range(gu_tiles):
        weight_copy(0, j).start(priority=1)
        weight_copy(1, j).start(priority=1)
    for j in range(d_tiles):
        weight_copy(2, j).start(priority=1)

    for load in loads:
        load.wait()
    own = pl.ds(pl.multiple_of(me * rows, rows), rows)
    tok = tokens_ref[...].astype(f32)
    inverse = lax.rsqrt(jnp.mean(tok * tok, axis=1, keepdims=True) + EPS)
    buf[own, :] = (tok * inverse * gain_ref[...]).astype(bf16)
    lanes = lax.broadcasted_iota(jnp.int32, (experts, rows), 0)
    spread = jnp.zeros((experts, rows), f32)
    for k in range(routes_ref.shape[0]):
        spread = spread + jnp.where(lanes == routes_ref[k:k + 1, :], rw_ref[k:k + 1, :], 0.0)
    meta[me, :, :rows] = spread[:experts // 2]
    meta[me, :, rows:] = spread[experts // 2:]

    pl.semaphore_wait(barrier, jnp.where(inner, 4, 3))

    def remote(src, dst, s, r, dev):
        return pltpu.make_async_remote_copy(
            src_ref=src, dst_ref=dst, send_sem=s, recv_sem=r, device_id={"ep": dev}, device_id_type=MESH
        )

    own_step = nz - 1

    def order(q):
        edge = 0 if 2 * q < nz else nz - 1
        far = nz - 1 - edge
        if q == edge:
            return sorted((p for p in range(nz) if p != q), key=lambda p: abs(p - q))
        return [edge] + [p for p in range(nz) if p not in (q, edge, far)] + [far]

    tables = [order(q) for q in range(nz)]
    places = []
    for i in range(own_step):
        value = tables[0][i]
        for q in range(1, nz):
            value = jnp.where(z == q, tables[q][i], value)
        places.append(value)
    places.append(z)

    def block_of(i, same_x, same_core):
        col = x if same_x else 1 - x
        lane = core if same_core else 1 - core
        return places[i] * 4 + col * 2 + lane

    def rows_of(i, same_x, same_core, q=None):
        at = block_of(i, same_x, same_core) * rows
        if q is None:
            return buf.at[pl.ds(pl.multiple_of(at, rows), rows), :]
        return buf.at[pl.ds(pl.multiple_of(at + q * sub, sub), sub), :]

    def piece(i, same_x, q):
        if q is META:
            return meta.at[block_of(i, same_x, True)]
        return rows_of(i, same_x, True, q)

    def slot_of(q):
        return pieces if q is META else q

    def ag_z(i, q, up):
        ref = piece(i, True, q)
        peer = me + 4 if up else me - 4
        return remote(ref, ref, sent.at[int(up) + (2 if q is META else 0)], az_r.at[places[i], slot_of(q)], peer)

    def ag_x(i, q, arriving=False):
        ref = piece(i, not arriving, q)
        return remote(ref, ref, sent.at[5 if q is META else 4], ax_r.at[i, slot_of(q)], x_peer)

    def ag_d(i, j, q):
        ref = piece(i, j == 0, q)
        r = md_r if q is META else ad_r
        return remote(ref, ref, sent.at[7 if q is META else 6], r.at[i, j], d_peer)

    def ag_d_all(i, j):
        ref = rows_of(i, j == 0, False)
        return remote(ref, ref, sent.at[6], ad_r.at[i, j], d_peer)

    def meta_arrives(i, j):
        ref = meta.at[block_of(i, j == 0, False)]
        remote(ref, ref, sent.at[7], md_r.at[i, j], d_peer).wait_recv()

    def sent_all(ref, n):
        remote(ref, ref, sent.at[n], sent.at[n], d_peer).wait_send()

    def gather_sent():
        for k in range(nz):
            @pl.when(z == k)
            def _():
                for up, blocks in ((0, nz - k if k > 0 else 0), (1, k + 1 if k < nz - 1 else 0)):
                    if blocks:
                        sent_all(buf.at[pl.ds(0, blocks * rows), :], up)
                        sent_all(meta.at[pl.ds(0, blocks)], up + 2)
        sent_all(buf.at[pl.ds(0, nz * rows), :], 4)
        sent_all(meta.at[pl.ds(0, nz)], 5)
        sent_all(buf.at[pl.ds(0, 2 * nz * rows), :], 6)
        sent_all(meta.at[pl.ds(0, 2 * nz)], 7)

    def start(copy):
        copy.start()

    def send_up(i, q, action):
        cond = has_above if i == own_step else jnp.logical_and(has_above, places[i] < z)
        pl.when(cond)(lambda: action(ag_z(i, q, True)))

    def send_down(i, q, action):
        cond = has_below if i == own_step else jnp.logical_and(has_below, places[i] > z)
        pl.when(cond)(lambda: action(ag_z(i, q, False)))

    def pass_on(i, q, action):
        send_up(i, q, action)
        send_down(i, q, action)

    def z_in(i, q):
        ag_z(i, q, True).wait_recv()
        pass_on(i, q, start)
        ag_d(i, 0, q).start()

    def x_out(i, q):
        ag_x(i, q).start()

    def x_in(i, q):
        ag_x(i, q, True).wait_recv()
        ag_d(i, 1, q).start()

    def rs_block(i, j, same_x):
        return part.at[i, j, x if same_x else 1 - x, core]

    def rs_d(i, j):
        return remote(part.at[i, j, :, 1 - core], dbuf.at[i, j], sent.at[8], rd_r.at[i, j], d_peer)

    def rs_x(i, j):
        return remote(rs_block(i, j, False), xbuf.at[i, j], sent.at[9], rx_r.at[i, j], x_peer)

    def rs_z(i, j):
        level, slot = places[i], z
        if i >= 1:
            level = jnp.where(outer, places[0], level)
            slot = jnp.where(outer, nz + i - 1, slot)
        peer = level * 4 + x * 2 + core
        return remote(rs_block(i, j, True), zbuf.at[slot, j], sent.at[10], rz_r.at[slot, j], peer)

    def rs_z_arriving(slot, j):
        ref = zbuf.at[slot, j]
        return remote(ref, ref, sent.at[10], rz_r.at[slot, j], x_peer)

    def chunk_rows(i):
        return pl.ds(pl.multiple_of(places[i] * chunk, chunk), chunk)

    def gate_up_rows(source, kept, target, j, width):
        cols = pl.ds(pl.multiple_of(j * width, width), width)
        lhs = buf[source, :]
        g = jnp.dot(lhs, wg[:, cols], preferred_element_type=f32)
        u = jnp.dot(lhs, wu[:, cols], preferred_element_type=f32)
        kept[target, cols] = (g / (1.0 + jnp.exp(-g)) * u).astype(bf16)

    def gate_up(i, j):
        gate_up_rows(chunk_rows(i), hid, pl.ds(0, chunk), j, 2 * tile)

    def gate_up_chip(j, col, fresh, i=own_step):
        if fresh:
            weight_copy(0, j).wait()
            weight_copy(1, j).wait()
        at = pl.multiple_of(col * (2 * rows), 2 * rows)
        start_row = pl.multiple_of(places[i] * chunk + col * (2 * rows), 2 * rows)
        gate_up_rows(pl.ds(start_row, 2 * rows), hid_own if i == own_step else hid, pl.ds(at, 2 * rows), j, tile)

    def weight_of(i):
        eye = lax.broadcasted_iota(jnp.int32, (rows, rows), 0) == lax.broadcasted_iota(jnp.int32, (rows, rows), 1)
        line, side = lax.rem(me, experts // 2), lax.div(me, experts // 2)
        cols = []
        for b in range(4):
            both = meta[places[i] * 4 + b, pl.ds(line, 1), :]
            row = jnp.where(side == 0, both[:, :rows], both[:, rows:])
            cols.append(jnp.sum(jnp.where(eye, row, 0.0), axis=1, keepdims=True))
        return jnp.concatenate(cols, axis=0)

    def down(i, duties, wide, begin=0, end=halves):
        weight = weight_of(i)
        kept = hid_own if i == own_step else hid

        def body(t, carry):
            cols = pl.ds(pl.multiple_of(t * wide * tile, wide * tile), wide * tile)
            for n in range(wide):
                if i == 0:
                    weight_copy(2, t * wide + n).wait()
            o = jnp.dot(kept[...], wd[:, cols], preferred_element_type=f32)
            for n in range(wide):
                value = (o[:, n * tile:(n + 1) * tile] * weight).astype(bf16)
                part[i, t * wide + n] = value.reshape(2, 2, rows, half)
            for n in range(wide):
                rs_d(i, t * wide + n).start()
            duties(t)
            return carry

        lax.fori_loop(begin // wide, end // wide, body, 0)

    def finish_d(i, j):
        rs_d(i, j).wait_recv()
        ref = rs_block(i, j, False)
        ref[...] = (ref[...].astype(f32) + dbuf[i, j, 1 - x].astype(f32)).astype(bf16)
        rs_x(i, j).start()

    def finish_x(i, j):
        rs_x(i, j).wait_recv()
        ref = rs_block(i, j, True)
        value = ref[...].astype(f32) + dbuf[i, j, x].astype(f32) + xbuf[i, j].astype(f32)
        if i == own_step:
            total[j] = value
        else:
            ref[...] = value.astype(bf16)
            if i >= 1:
                @pl.when(inner)
                def _():
                    rs_z_arriving(nz + i - 1, j).wait_recv()
                    ref[...] = (value + zbuf[nz + i - 1, j].astype(f32)).astype(bf16)
            rs_z(i, j).start()

    def loop(i, duties):
        def body(j, carry):
            gate_up(i, j)
            duties(j)
            return carry

        lax.fori_loop(0, gu_tiles // 2, body, 0)

    def chunk_ready(i):
        for j in range(2):
            ag_d_all(i, j).wait_recv()

    def step(body):
        lax.fori_loop(0, pieces, lambda j, carry: (body(j), carry)[1], 0)

    for q in [META] + list(range(pieces)):
        x_out(own_step, q)
        pass_on(own_step, q, start)
        ag_d(own_step, 0, q).start()

    z_in(0, META)
    x_out(0, META)

    @pl.when(inner)
    def _():
        z_in(1, META)
        x_out(1, META)

    ag_d_all(own_step, 0).wait_recv()

    def gather(q):
        gate_up_chip(q, x, True)
        x_in(own_step, q)
        z_in(0, q)
        x_out(0, q)
        pl.when(inner)(lambda: z_in(1, q))

    step(gather)

    @pl.when(inner)
    def _():
        z_in(2, META)
        x_out(2, META)

    @pl.when(outer)
    def _():
        z_in(1, META)
        x_out(1, META)

    ag_d_all(own_step, 1).wait_recv()

    def own_rest(j):
        gate_up_chip(j, 1 - x, False)
        pl.when(inner)(lambda: z_in(2, j))
        pl.when(outer)(lambda: z_in(1, j))
        x_out(1, j)
        x_in(0, j)
        pl.when(j == 0)(lambda: ag_d_all(0, 0).wait_recv())
        gate_up_chip(j, x, False, 0)

    step(own_rest)

    @pl.when(inner)
    def _():
        for q in range(pieces):
            x_out(2, q)

    @pl.when(outer)
    def _():
        z_in(2, META)
        x_out(2, META)

    x_in(own_step, META)
    x_in(0, META)
    ag_d_all(0, 1).wait_recv()

    def both(action, j):
        action(2 * j)
        action(2 * j + 1)

    def far_in(q):
        z_in(2, q)
        x_out(2, q)

    def near_rest(j):
        gate_up_chip(j, 1 - x, False, 0)
        pl.when(outer)(lambda: far_in(j))
        pl.when(j >= 1)(lambda: x_in(1, j - 1))

    step(near_rest)
    for j in range(2):
        meta_arrives(0, j)

    def down_duties_0(t):
        pl.when(t == 0)(lambda: x_in(1, 3))

    down(0, down_duties_0, 2)
    x_in(1, META)
    chunk_ready(1)

    def duties_1(j):
        both(lambda q: finish_d(0, q), j)
        both(lambda q: x_in(2, q), j)

    loop(1, duties_1)
    x_in(2, META)
    for j in range(2):
        meta_arrives(1, j)

    def down_duties_1(t):
        pl.when(t == 1)(lambda: both(lambda j: finish_d(1, j), 0))
        pl.when(t == 1)(lambda: both(lambda j: finish_x(0, j), 0))

    down(1, down_duties_1, 2)
    chunk_ready(2)

    def duties_2(j):
        @pl.when(j == 0)
        def _():
            both(lambda q: finish_d(1, q), 1)
            both(lambda q: finish_x(0, q), 1)

        pl.when(jnp.logical_and(j == 1, outer))(lambda: finish_x(1, 0))

    loop(2, duties_2)
    for i in (2, own_step):
        for j in range(2):
            meta_arrives(i, j)

    def down_duties_2(t):
        pl.when(t >= 2)(lambda: finish_d(2, t - 2))
        pl.when(jnp.logical_and(t < 3, outer))(lambda: finish_x(1, t + 1))

    down(2, down_duties_2, 1)

    def down_duties_own(t):
        pl.when(t < 2)(lambda: finish_d(2, t + 2))
        pl.when(t >= 2)(lambda: finish_d(own_step, t - 2))
        pl.when(inner)(lambda: finish_x(1, t))

    down(own_step, down_duties_own, 1)
    finish_x(2, 0)
    finish_d(own_step, 2)
    finish_x(2, 1)
    finish_d(own_step, 3)
    finish_x(2, 2)
    finish_x(2, 3)
    gather_sent()
    step(lambda j: finish_x(own_step, j))

    def collect(level, cond):
        def one(j):
            rs_z_arriving(level, j).wait_recv()
            total[j] = total[j] + zbuf[level, j].astype(f32)

        pl.when(cond)(lambda: step(one))

    for level in range(nz):
        if level in (0, nz - 1):
            collect(level, z == (1 if level == 0 else nz - 2))
        else:
            collect(level, z != level)

    squares = 0.0
    for j in range(halves):
        squares = squares + jnp.sum(total[j] * total[j], axis=1, keepdims=True)
    inverse_out = lax.rsqrt(squares / features + EPS)
    for j in range(halves):
        cols = pl.ds(j * half, half)
        out_ref[:, cols] = (total[j] * inverse_out * fgain_ref[:, cols]).astype(out_ref.dtype)

    sent_all(dbuf, 8)
    sent_all(xbuf, 9)
    sent_all(zbuf.at[pl.ds(0, own_step)], 10)


def fused_device(tokens, norm_gain, routes, route_weights, w_gate, w_up, w_down, final_gain):
    rows, features = tokens.shape
    hidden_units = w_gate.shape[2]
    experts = lax.axis_size("ep")
    nz = experts // 4
    pieces, halves = 4, 4
    tile = hidden_units // pieces
    half = features // halves
    vmem, hbm = pl.BlockSpec(memory_space=pltpu.VMEM), pl.BlockSpec(memory_space=pltpu.HBM)
    dma = pltpu.SemaphoreType.DMA
    bf16 = jnp.bfloat16
    return pl.pallas_call(
        functools.partial(fused_kernel, nz, tile, pieces),
        out_shape=jax.ShapeDtypeStruct((rows, features), jnp.bfloat16),
        in_specs=[hbm] * 8,
        out_specs=vmem,
        scratch_shapes=[
            pltpu.VMEM((rows, features), bf16),
            pltpu.VMEM((1, features), jnp.float32),
            pltpu.VMEM(routes.shape[::-1], jnp.int32),
            pltpu.VMEM(routes.shape[::-1], jnp.float32),
            pltpu.VMEM((1, features), jnp.float32),
            dma((5,)),
            pltpu.VMEM((experts * rows, features), bf16),
            pltpu.VMEM((features, hidden_units), bf16),
            pltpu.VMEM((features, hidden_units), bf16),
            pltpu.VMEM((hidden_units, features), bf16),
            pltpu.VMEM((4 * rows, hidden_units), bf16),
            pltpu.VMEM((4 * rows, hidden_units), bf16),
            pltpu.VMEM((nz, halves, 2, 2, rows, half), bf16),
            pltpu.VMEM((nz, halves, 2, rows, half), bf16),
            pltpu.VMEM((nz, halves, rows, half), bf16),
            pltpu.VMEM((nz + 2, halves, rows, half), bf16),
            pltpu.VMEM((halves, rows, half), jnp.float32),
            pltpu.VMEM((experts, experts // 2, 2 * rows), jnp.float32),
            dma((3, max(hidden_units, features) // tile)),
            dma((11,)), dma((nz, pieces + 1)), dma((nz, pieces + 1)), dma((nz, 2)), dma((nz, 2)),
            dma((nz, halves)), dma((nz, halves)), dma((nz + 2, halves)),
        ],
        compiler_params=pltpu.CompilerParams(
            collective_id=0, has_side_effects=True, vmem_limit_bytes=48 * 1024 * 1024
        ),
    )(*(
        pltpu.with_memory_space_constraint(array, pltpu.HBM)
        for array in (
            tokens, norm_gain[None, :], routes.T, route_weights.T, w_gate, w_up, w_down, final_gain[None, :],
        )
    ))


def solution(mesh):
    placed = (
        P(("grp", "ep"), None),
        P(),
        P(("grp", "ep"), None),
        P(("grp", "ep"), None),
        P("ep", None, "tp"),
        P("ep", None, "tp"),
        P("ep", "tp", None),
        P("tp"),
    )
    ep, tp = mesh.shape["ep"], mesh.shape["tp"]

    def step(*args):
        rows, features = args[0].shape
        hidden_units = args[4].shape[2]
        fits = 3 * features * hidden_units + 3 * ep * rows * features < 24 * 2 ** 20
        whole_tiles = features % 2048 == 0 and hidden_units % 2048 == 0 and rows % 64 == 0
        if tp == 1 and ep == 16 and args[4].shape[0] == 1 and fits and whole_tiles:
            return fused_device(*args)
        return per_device(*args)

    return jax.shard_map(
        step, mesh=mesh, in_specs=placed, out_specs=P(("grp", "ep"), "tp"), check_vma=False
    )
```
